32 devices in a mesh: sp: 8 (over z, y), tp: 4 (over x, core).
Axes of the slice: x: 2, y: 2, z: 4, core: 2. Of those that a mesh axis runs over, the one named last changes fastest.
Arguments:
- mixer_input: bfloat16 [4096, 1024], P('sp', 'tp'), may hold values from -6 to 6
- residual: bfloat16 [4096, 2048], P(('sp', 'tp')), may hold values from -6 to 6
- decay_real: float32 [64, 64], P('tp'), may hold values from -0.07 to 0
- decay_imag: float32 [64, 64], P('tp'), may hold values from 0.3 to 3
- log_step: float32 [64], P('tp'), may hold values from -0.7 to 0.7
- input_re: float32 [64, 64, 16], P('tp'), may hold values from -1.5 to 1.5
- input_im: float32 [64, 64, 16], P('tp'), may hold values from -1.5 to 1.5
- output_re: float32 [64, 16, 64], P('tp'), may hold values from -0.5 to 0.5
- output_im: float32 [64, 16, 64], P('tp'), may hold values from -0.5 to 0.5
- skip_gain: float32 [64, 16], P('tp'), may hold values from -4 to 4
- glu_weight: bfloat16 [1024, 1024], replicated, may hold values from -0.1875 to 0.1875
- glu_bias: float32 [1024], replicated, may hold values from -4 to 4
- mix_gain: float32 [1024], replicated, may hold values from 0.1 to 1.9
- out_weight: bfloat16 [1024, 2048], replicated, may hold values from -0.1875 to 0.1875
- norm_gain: float32 [2048], replicated, may hold values from 0.1 to 1.9
- route_ids: int32 [4096, 4], P(('sp', 'tp')), may hold values from 0 to 31, all different within a row; in each aligned block of 128 rows (0 to 127, 128 to 255, ...) at most 24 rows name the same one
- route_gates: float32 [4096, 4], P(('sp', 'tp')), may hold values from 0.25 to 1
- expert_gate: bfloat16 [32, 2048, 512], P(('sp', 'tp')), may hold values from -0.125 to 0.125
- expert_up: bfloat16 [32, 2048, 512], P(('sp', 'tp')), may hold values from -0.125 to 0.125
- expert_down: bfloat16 [32, 512, 2048], P(('sp', 'tp')), may hold values from -0.25 to 0.25
- shared_gate: bfloat16 [2048, 512], replicated, may hold values from -0.125 to 0.125
- shared_up: bfloat16 [2048, 512], replicated, may hold values from -0.125 to 0.125
- shared_down: bfloat16 [512, 2048], replicated, may hold values from -0.25 to 0.25
Outputs:
- layer_out: bfloat16 [4096, 2048], P(('sp', 'tp'))
The draws below stay inside these ranges and needn't reach their ends.
Inputs may be any that keep to these rules, and one draw needn't show every extreme that they name: `route_ids`: each row names 4 different experts; among the 128 rows of one device no expert is named by more than 24 rows, and in every draw some expert is named by exactly 24 of them.
All inputs are finite; a program needn't handle non-finite values.
Results may differ from the reference program's by a relative error of at most 0.018.
Values may be sent and summed in bfloat16 or wider, within the bound.
A program may use at most 128 MiB of HBM per device.

```python
import math
import jax
import jax.numpy as jnp
import numpy as np
from jax import lax

D = 2048
GROUPS = 64
CH = 16
STATE = 64
FF = 512
TOPK = 4
TOK_SP = 512
WIDTH = 1024
TOKENS = 4096
ROWS = 128
EXPERTS = 32
CAP = 24
N_SP = 8


def slow_groups(key, slow_share):
    return jax.random.uniform(jax.random.fold_in(key, 101), (GROUPS,)) < slow_share


def input_part(key, salt_value, slow_share):
    is_slow = slow_groups(key, slow_share)
    values = jnp.clip(jax.random.normal(jax.random.fold_in(key, salt_value), (GROUPS, STATE, CH), jnp.float32), -6.0, 6.0)
    scaling = jnp.where(is_slow, jnp.sqrt(50.0 / TOKENS), 1.0) * (2.0 * CH) ** (-0.5)
    return values * scaling[:, None, None]


def draw_decay_real(key, part):
    slow_share = 0.5
    is_slow = slow_groups(key, slow_share)
    picked = jax.random.uniform(jax.random.fold_in(key, 1), (GROUPS, STATE), jnp.float32)
    slow_rate = jnp.exp(jnp.log(0.05) + picked * jnp.log(10.0)) / TOKENS
    fast_rate = jnp.exp(jnp.log(1.0 / 50.0) + picked * jnp.log(50.0 / 15.0))
    return -jnp.where(is_slow[:, None], slow_rate, fast_rate)


def draw_input_re(key, part):
    slow_share = 0.5
    return input_part(key, 3, slow_share)


def draw_input_im(key, part):
    slow_share = 0.5
    return input_part(key, 4, slow_share)


def shard_levels(rng, extent, pieces, low, top_value):
    level = 1.0
    for dim, blocks in pieces:
        steps = jax.random.uniform(jax.random.fold_in(jax.random.fold_in(rng, 6), dim), (blocks,), jnp.float32, low / len(pieces), top_value / len(pieces))
        level = level * jnp.repeat(jnp.exp(steps), extent[dim] // blocks).reshape((-1,) + (1,) * (len(extent) - 1 - dim))
    return level


def deal_out(own_key, own, number, rows, number_of, top, reach, skew):
    order = jax.random.permutation(own_key, number_of)
    heavy_load, common = shares(number_of, rows * top, reach, skew, True), shares(number_of, rows * top, reach, skew, False)
    places = jnp.arange(number_of)

    def named(tallies, rotation):
        used = int((tallies > 0).sum())
        fixed = max(1, used // 4)
        shifted = fixed + (places - fixed + rotation * (used - fixed)) % max(1, number_of - fixed)
        return jnp.zeros((number_of,), jnp.int32).at[order[jnp.where(places < fixed, places, shifted)]].set(jnp.asarray(tallies, jnp.int32))

    tallies = jnp.where(number % 4 == 0, named(heavy_load, number // 4), named(common, number - number // 4 - 1))
    mixed = jax.random.permutation(jax.random.fold_in(own, 3), number_of)
    giver, sink = mixed[0:number_of // 2 * 2:2], mixed[1:number_of // 2 * 2:2]
    slack = jnp.minimum(tallies[giver] - 1, reach - tallies[sink]) // 2
    slack = jnp.where((giver == order[0]) | (sink == order[0]) | (tallies[sink] == 0), 0, jnp.maximum(slack, 0))
    shifted = jax.random.randint(jax.random.fold_in(own, 4), (number_of // 2,), 0, 1 << 20) % (slack + 1)
    tallies = tallies.at[giver].add(-shifted).at[sink].add(shifted)
    labels = jnp.searchsorted(jnp.cumsum(tallies), jnp.arange(rows * top), side="right").astype(jnp.int32)
    table = labels.reshape(top, rows).T
    table = table[jax.random.permutation(jax.random.fold_in(own, 1), rows)]
    rotation = jax.random.randint(jax.random.fold_in(own, 2), (rows, 1), 0, top)
    return jnp.take_along_axis(table, (jnp.arange(top)[None, :] + rotation) % top, axis=1)


def shares(number_of, total, limit, skew, full):
    portions = [(1 << 20) // math.isqrt(grade ** skew) + 1 for grade in range(1, number_of + 1)]
    largest = limit if full else min(limit, max(-(-total // number_of), total * portions[0] // sum(portions)))
    least = 1 if total - largest >= number_of - 1 else 0
    counts, spare = [largest] + [least] * (number_of - 1), total - largest - least * (number_of - 1)
    while spare > 0:
        movable = [i for i in range(1, number_of) if counts[i] < largest] or [i for i in range(1, number_of) if counts[i] < limit]
        mass, left = sum([portions[i] for i in movable]), spare
        for i in movable:
            extra = min(limit - counts[i], max(1, left * portions[i] // mass), spare)
            counts[i] = counts[i] + extra
            spare = spare - extra
    return np.array(counts)


def bell_draw(rng, extent, scale, reach, pieces=(), held_as=jnp.bfloat16):
    entries = scale * jax.random.normal(rng, extent, jnp.float32)
    if pieces:
        entries = entries * shard_levels(rng, extent, pieces, -0.22, 0.18)
    return jnp.clip(entries, -reach, reach).astype(held_as)


def setup_inputs(seed: int = 0) -> dict:
    seeds = jax.random.split(jax.random.key(seed), 24)
    mixer_input = bell_draw(seeds[0], (TOKENS, WIDTH), 1.0, 6.0, ((0, 8), (1, 4)))
    residual = bell_draw(seeds[1], (TOKENS, D), 1.0, 6.0, ((0, 32),))
    decay_real = draw_decay_real(jax.random.fold_in(seeds[23], 71), 0)
    decay_imag = jnp.clip(0.3 + 2.7 * jax.random.uniform(seeds[3], (GROUPS, STATE), jnp.float32) ** shard_levels(seeds[3], (GROUPS, STATE), ((0, 4),), -0.2, 0.2), 0.3, 3.0)
    log_step = jnp.clip(jax.random.uniform(seeds[4], (GROUPS,), jnp.float32, -0.7, 0.7) * shard_levels(seeds[4], (GROUPS,), ((0, 4),), -0.4, 0.0), -0.7, 0.7)
    input_re = draw_input_re(jax.random.fold_in(seeds[23], 71), 0)
    input_im = draw_input_im(jax.random.fold_in(seeds[23], 71), 0)
    output_re = bell_draw(seeds[7], (GROUPS, CH, STATE), (2 * STATE) ** -0.5, 0.5, ((0, 4),), jnp.float32)
    output_im = bell_draw(seeds[8], (GROUPS, CH, STATE), (2 * STATE) ** -0.5, 0.5, ((0, 4),), jnp.float32)
    skip_gain = bell_draw(seeds[9], (GROUPS, CH), 1.0, 4.0, ((0, 4),), jnp.float32)
    glu_weight = bell_draw(seeds[10], (WIDTH, WIDTH), WIDTH ** -0.5, 0.1875)
    glu_bias = bell_draw(seeds[11], (WIDTH,), 1.0, 4.0, (), jnp.float32)
    mix_gain = jnp.clip(1.0 + 0.18 * jax.random.normal(seeds[12], (WIDTH,), jnp.float32), 0.1, 1.9)
    out_weight = bell_draw(seeds[13], (WIDTH, D), WIDTH ** -0.5, 0.1875)
    norm_gain = jnp.clip(1.0 + 0.18 * jax.random.normal(seeds[14], (D,), jnp.float32), 0.1, 1.9)
    route_ids_keys = jax.random.split(jax.random.fold_in(seeds[15], 1), TOKENS // ROWS)
    route_ids_turns = jax.random.permutation(jax.random.fold_in(seeds[15], 3), TOKENS // ROWS)
    route_ids = jax.vmap(lambda own, number: deal_out(jax.random.fold_in(seeds[15], 2), own, number, ROWS, EXPERTS, TOPK, CAP, 2))(route_ids_keys, route_ids_turns).reshape((TOKENS, TOPK))
    route_gates = jnp.clip(0.25 + 0.75 * jax.random.uniform(seeds[16], (TOKENS, TOPK), jnp.float32) ** shard_levels(seeds[16], (TOKENS, TOPK), ((0, 32),), -0.2, 0.2), 0.25, 1.0)
    expert_gate = bell_draw(seeds[17], (EXPERTS, D, FF), D ** -0.5, 0.125, ((0, 32),))
    expert_up = bell_draw(seeds[18], (EXPERTS, D, FF), D ** -0.5, 0.125, ((0, 32),))
    expert_down = bell_draw(seeds[19], (EXPERTS, FF, D), FF ** -0.5, 0.25, ((0, 32),))
    shared_gate = bell_draw(seeds[20], (D, FF), D ** -0.5, 0.125)
    shared_up = bell_draw(seeds[21], (D, FF), D ** -0.5, 0.125)
    shared_down = bell_draw(seeds[22], (FF, D), FF ** -0.5, 0.25)
    return {"mixer_input": mixer_input, "residual": residual, "decay_real": decay_real, "decay_imag": decay_imag, "log_step": log_step, "input_re": input_re, "input_im": input_im, "output_re": output_re, "output_im": output_im, "skip_gain": skip_gain, "glu_weight": glu_weight, "glu_bias": glu_bias, "mix_gain": mix_gain, "out_weight": out_weight, "norm_gain": norm_gain, "route_ids": route_ids, "route_gates": route_gates, "expert_gate": expert_gate, "expert_up": expert_up, "expert_down": expert_down, "shared_gate": shared_gate, "shared_up": shared_up, "shared_down": shared_down}


NORM_EPS = 1e-06
HIGHEST = lax.Precision.HIGHEST

def discretize(decay_real, decay_imag, log_step, input_re, input_im):
    step_size = jnp.exp(log_step)[:, None]
    log_rate = decay_real * step_size
    turn_angle = decay_imag * step_size
    bar_re = jnp.exp(log_rate) * jnp.cos(turn_angle)
    bar_im = jnp.exp(log_rate) * jnp.sin(turn_angle)
    denominator = decay_real * decay_real + decay_imag * decay_imag
    less_one = bar_re - 1.0
    coef_re = (less_one * decay_real + bar_im * decay_imag) / denominator
    coef_im = (bar_im * decay_real - less_one * decay_imag) / denominator
    drive_re = coef_re[:, :, None] * input_re - coef_im[:, :, None] * input_im
    drive_im = coef_re[:, :, None] * input_im + coef_im[:, :, None] * input_re
    return (log_rate.reshape(-1), turn_angle.reshape(-1), jnp.concatenate([drive_re, drive_im], axis=1))

def powers(count, log_rate, turn_angle):
    magnitude = jnp.exp(count * log_rate)
    return (magnitude * jnp.cos(count * turn_angle), magnitude * jnp.sin(count * turn_angle))

def local_states(inputs, drive, log_rate, turn_angle):
    length, width_all = inputs.shape
    group_count = drive.shape[0]
    channels = width_all // group_count
    state_count = drive.shape[1] // 2
    driven = jnp.einsum('lgc,gnc->lgn', inputs.astype(jnp.float32).reshape(length, group_count, channels), drive, precision=HIGHEST)
    state_re = driven[:, :, :state_count].reshape(length, group_count * state_count)
    state_im = driven[:, :, state_count:].reshape(length, group_count * state_count)
    offset = 1
    while offset < length:
        pow_re, pow_im = powers(float(offset), log_rate, turn_angle)
        prior_re = jnp.pad(state_re[:-offset], ((offset, 0), (0, 0)))
        prior_im = jnp.pad(state_im[:-offset], ((offset, 0), (0, 0)))
        state_re, state_im = (state_re + pow_re * prior_re - pow_im * prior_im, state_im + pow_re * prior_im + pow_im * prior_re)
        offset *= 2
    return (state_re, state_im)

def read_out(state_re, state_im, output_re, output_im):
    length = state_re.shape[0]
    group_count, channels, state_count = output_re.shape
    stacked = jnp.concatenate([state_re.reshape(length, group_count, state_count), state_im.reshape(length, group_count, state_count)], axis=2)
    table = jnp.concatenate([output_re, -output_im], axis=2)
    return jnp.einsum('lgn,gcn->lgc', stacked, table, precision=HIGHEST).reshape(length, group_count * channels)

def rms_scale(values, gain):
    return values * lax.rsqrt(lax.optimization_barrier(jnp.mean(values * values, axis=-1, keepdims=True)) + NORM_EPS) * gain

def reference(mixer_input, residual, decay_real, decay_imag, log_step, input_re, input_im, output_re, output_im, skip_gain, glu_weight, glu_bias, mix_gain, out_weight, norm_gain, route_ids, route_gates, expert_gate, expert_up, expert_down, shared_gate, shared_up, shared_down):
    log_rate, turn_angle, drive = discretize(decay_real, decay_imag, log_step, input_re, input_im)
    blocks = mixer_input.reshape(N_SP, TOK_SP, WIDTH)
    positions = jnp.arange(1, TOK_SP + 1, dtype=jnp.float32)[:, None]
    pow_re, pow_im = powers(positions, log_rate, turn_angle)

    def advance(carry_state, block_input):
        state_re, state_im = local_states(block_input, drive, log_rate, turn_angle)
        full_re = state_re + pow_re * carry_state[0] - pow_im * carry_state[1]
        full_im = state_im + pow_re * carry_state[1] + pow_im * carry_state[0]
        readout = read_out(full_re, full_im, output_re, output_im)
        mixed = jax.nn.gelu(readout + skip_gain.reshape(-1) * block_input.astype(jnp.float32))
        return ((full_re[-1], full_im[-1]), mixed.astype(jnp.bfloat16))
    start = (jnp.zeros_like(log_rate), jnp.zeros_like(log_rate))
    mixed = lax.scan(advance, start, blocks)[1].reshape(TOKENS, WIDTH)
    pre_gate = jnp.dot(mixed, glu_weight, preferred_element_type=jnp.float32) + glu_bias
    gated = mixed.astype(jnp.float32) * jax.nn.sigmoid(pre_gate)
    normed = rms_scale(gated, mix_gain).astype(jnp.bfloat16)
    stream = residual.astype(jnp.float32) + jnp.dot(normed, out_weight, preferred_element_type=jnp.float32)
    hidden_in = rms_scale(stream, norm_gain).astype(jnp.bfloat16)
    shared_hidden = (jax.nn.silu(jnp.dot(hidden_in, shared_gate, preferred_element_type=jnp.float32)) * jnp.dot(hidden_in, shared_up, preferred_element_type=jnp.float32)).astype(jnp.bfloat16)
    total = stream + jnp.dot(shared_hidden, shared_down, preferred_element_type=jnp.float32)
    flat_ids = route_ids.reshape(-1)
    flat_gates = route_gates.reshape(-1)
    slot_count = EXPERTS * CAP

    def one_expert(routed, expert):
        missing = (flat_ids != expert).astype(jnp.int32)
        ordering = jnp.argsort(missing, stable=True)[:slot_count].astype(jnp.int32)
        is_valid = flat_ids[ordering] == expert
        token_idx = (ordering // TOPK).astype(jnp.int32)
        rows_in = hidden_in[token_idx]
        gate_w = lax.dynamic_index_in_dim(expert_gate, expert, 0, keepdims=False)
        up_w = lax.dynamic_index_in_dim(expert_up, expert, 0, keepdims=False)
        down_w = lax.dynamic_index_in_dim(expert_down, expert, 0, keepdims=False)
        hidden = (jax.nn.silu(jnp.dot(rows_in, gate_w, preferred_element_type=jnp.float32)) * jnp.dot(rows_in, up_w, preferred_element_type=jnp.float32)).astype(jnp.bfloat16)
        expert_out = jnp.dot(hidden, down_w, preferred_element_type=jnp.float32).astype(jnp.bfloat16)
        weight = jnp.where(is_valid, flat_gates[ordering], jnp.zeros_like(flat_gates[ordering]))
        return (routed.at[token_idx].add(weight[:, None] * expert_out.astype(jnp.float32)), None)
    routed = lax.scan(one_expert, jnp.zeros((TOKENS, D), jnp.float32), jnp.arange(EXPERTS, dtype=jnp.int32))[0]
    return (total + routed).astype(jnp.bfloat16)
```

```python
import functools
import math

import jax
import jax.numpy as jnp
from jax import lax
from jax.experimental import pallas as pl
from jax.experimental.pallas import tpu as pltpu
from jax.sharding import PartitionSpec as P

NORM_EPS = 1e-06
HIGHEST = lax.Precision.HIGHEST
MESH = pl.DeviceIdType.MESH


def exchange_kernel(count, position, member, same, block_ref, out_ref, send_sem, recv_sem, own_sem):
    me = position()
    barrier = pltpu.get_barrier_semaphore()

    def greet(step, carry):
        pl.semaphore_signal(
            barrier, inc=1, device_id=member(lax.rem(me + step, count)), device_id_type=MESH
        )
        return carry

    stride = 7 if math.gcd(7, count - 1) == 1 else 1

    def copy(step):
        ahead = 1 + lax.rem((step - 1) * stride + count // 4, count - 1)
        to = lax.rem(me + ahead, count)
        return pltpu.make_async_remote_copy(
            src_ref=block_ref if same else block_ref.at[to],
            dst_ref=out_ref.at[me],
            send_sem=send_sem.at[step],
            recv_sem=recv_sem.at[step],
            device_id=member(to),
            device_id_type=MESH,
        )

    def begin(step, carry):
        copy(step).start()
        return carry

    def finish(step, carry):
        copy(step).wait()
        return carry

    own = pltpu.make_async_copy(block_ref if same else block_ref.at[me], out_ref.at[me], own_sem)
    own.start()
    lax.fori_loop(1, count, greet, 0)
    pl.semaphore_wait(barrier, count - 1)
    lax.fori_loop(1, count, begin, 0)
    lax.fori_loop(1, count, finish, 0)
    own.wait()


def exchange(block, count, position, member, collective_id, same=False):
    shape = (count,) + block.shape if same else block.shape
    return pl.pallas_call(
        functools.partial(exchange_kernel, count, position, member, same),
        out_shape=jax.ShapeDtypeStruct(shape, block.dtype),
        in_specs=[pl.BlockSpec(memory_space=pl.ANY)],
        out_specs=pl.BlockSpec(memory_space=pl.ANY),
        scratch_shapes=[
            pltpu.SemaphoreType.DMA((count,)),
            pltpu.SemaphoreType.DMA((count,)),
            pltpu.SemaphoreType.DMA,
        ],
        compiler_params=pltpu.CompilerParams(collective_id=collective_id, has_side_effects=True),
    )(block)


def gather_sp(block):
    return exchange(
        block,
        lax.axis_size("sp"),
        lambda: lax.axis_index("sp"),
        lambda index: (index, lax.axis_index("tp")),
        1,
        same=True,
    )


def exchange_tp(block):
    return exchange(
        block,
        lax.axis_size("tp"),
        lambda: lax.axis_index("tp"),
        lambda index: (lax.axis_index("sp"), index),
        2,
    )


def planes_of(sp_count):
    return math.gcd(sp_count, 4)


def visiting_order(planes):
    return [sorted(range(planes), key=lambda other: (abs(other - own), -other)) for own in range(planes)]


def moe_kernel(
    sp_count,
    tp_count,
    capacity,
    routes_ref,
    hidden_ref,
    stream_ref,
    gate_hbm,
    up_hbm,
    down_hbm,
    sgate_hbm,
    sup_hbm,
    sdown_hbm,
    out_ref,
    blocks,
    sent,
    arrived,
    replies,
    returned,
    partial,
    homed,
    mix_weights,
    wide,
    total,
    gate_w,
    up_w,
    down_w,
    sgate_w,
    sup_w,
    sdown_w,
    weight_sem,
    own_sem,
    up_sem,
    down_sem,
    block_sem,
    sent_sem,
    arrived_sem,
    replies_sem,
    returned_sem,
    partial_sem,
    homed_sem,
):
    planes = planes_of(sp_count)
    rows_y = sp_count // planes
    members = rows_y * tp_count
    row_count, width = hidden_ref.shape
    hidden_width = gate_w.shape[1]
    slots = members * capacity
    top_count = routes_ref.shape[1] // 2
    column = min(512, width)
    sp = lax.axis_index("sp")
    tp = lax.axis_index("tp")
    plane = sp // rows_y
    row_y = lax.rem(sp, rows_y)
    me = row_y * tp_count + tp

    def member_id(other):
        return (plane * rows_y + other // tp_count, lax.rem(other, tp_count))

    def plane_id(other):
        return (other * rows_y + row_y, tp)

    loads = [
        pltpu.make_async_copy(source.at[0] if len(source.shape) == 3 else source, target, weight_sem.at[number])
        for number, (source, target) in enumerate(
            (
                (sgate_hbm, sgate_w),
                (sup_hbm, sup_w),
                (sdown_hbm, sdown_w),
                (gate_hbm, gate_w),
                (up_hbm, up_w),
                (down_hbm, down_w),
            )
        )
    ]
    barrier = pltpu.get_barrier_semaphore()

    def greet_member(step, carry):
        pl.semaphore_signal(
            barrier, inc=1, device_id=member_id(lax.rem(me + step, members)), device_id_type=MESH
        )
        return carry

    def greet_plane(step, carry):
        pl.semaphore_signal(
            barrier, inc=1, device_id=plane_id(lax.rem(plane + step, planes)), device_id_type=MESH
        )
        return carry

    lax.fori_loop(1, members, greet_member, 0)
    lax.fori_loop(1, planes, greet_plane, 0)
    for load in loads:
        load.start()
    blocks[plane] = hidden_ref[...]

    order = visiting_order(planes)

    def visited(step):
        block = jnp.int32(order[0][step])
        for own in range(1, planes):
            block = jnp.where(plane == own, order[own][step], block)
        return block

    steps = [plane] + [visited(step) for step in range(1, planes)]

    def pass_up(block):
        return pltpu.make_async_remote_copy(
            src_ref=blocks.at[block],
            dst_ref=blocks.at[block],
            send_sem=up_sem.at[block],
            recv_sem=block_sem.at[block],
            device_id=plane_id(jnp.minimum(plane + 1, planes - 1)),
            device_id_type=MESH,
        )

    def pass_down(block):
        return pltpu.make_async_remote_copy(
            src_ref=blocks.at[block],
            dst_ref=blocks.at[block],
            send_sem=down_sem.at[block],
            recv_sem=block_sem.at[block],
            device_id=plane_id(jnp.maximum(plane - 1, 0)),
            device_id_type=MESH,
        )

    def goes_up(block):
        return jnp.logical_and(block <= plane, plane < planes - 1)

    def goes_down(block):
        return jnp.logical_and(block >= plane, plane > 0)

    def forward(block):
        @pl.when(goes_up(block))
        def _():
            pass_up(block).start()

        @pl.when(goes_down(block))
        def _():
            pass_down(block).start()

    def deal(block, other):
        return pltpu.make_async_remote_copy(
            src_ref=sent.at[block, other],
            dst_ref=arrived.at[block, me],
            send_sem=sent_sem.at[block, other],
            recv_sem=arrived_sem.at[block, me],
            device_id=member_id(other),
            device_id_type=MESH,
        )

    def reply(block, other):
        return pltpu.make_async_remote_copy(
            src_ref=replies.at[block, other],
            dst_ref=returned.at[block, me],
            send_sem=replies_sem.at[block, other],
            recv_sem=returned_sem.at[block, me],
            device_id=member_id(other),
            device_id_type=MESH,
        )

    def landing(buffer, sem, block, other):
        return pltpu.make_async_remote_copy(
            src_ref=buffer.at[block, other],
            dst_ref=buffer.at[block, other],
            send_sem=sent_sem.at[block, other],
            recv_sem=sem.at[block, other],
            device_id=member_id(other),
            device_id_type=MESH,
        )

    def homeward(block):
        return pltpu.make_async_remote_copy(
            src_ref=partial.at[block],
            dst_ref=homed.at[plane],
            send_sem=partial_sem.at[block],
            recv_sem=homed_sem.at[plane],
            device_id=plane_id(block),
            device_id_type=MESH,
        )

    def each_other(action):
        def body(step, carry):
            action(lax.rem(me + step, members))
            return carry

        lax.fori_loop(1, members, body, 0)

    def place(block):
        routes = routes_ref[block * rows_y + row_y]
        experts = (lax.broadcasted_iota(jnp.int32, (members, row_count), 0) + plane * members).astype(
            jnp.float32
        )
        named = jnp.zeros((members, row_count), jnp.float32)
        gates = jnp.zeros((members, row_count), jnp.float32)
        for index in range(top_count):
            hit = experts == routes[index : index + 1, :]
            named = named + jnp.where(hit, 1.0, 0.0)
            gates = gates + jnp.where(hit, routes[top_count + index : top_count + index + 1, :], 0.0)
        before = (
            lax.broadcasted_iota(jnp.int32, (row_count, row_count), 0)
            < lax.broadcasted_iota(jnp.int32, (row_count, row_count), 1)
        )
        ranks = jnp.dot(
            named.astype(jnp.bfloat16),
            jnp.where(before, 1.0, 0.0).astype(jnp.bfloat16),
            preferred_element_type=jnp.float32,
        )
        ranks = jnp.where(named > 0.5, ranks, -1.0)
        numbers = lax.broadcasted_iota(jnp.int32, (capacity, row_count), 0).astype(jnp.float32)
        hits = [ranks[other : other + 1, :] == numbers for other in range(members)]
        picked = jnp.concatenate([jnp.where(hit, 1.0, 0.0) for hit in hits], axis=0)
        scaled = jnp.concatenate(
            [jnp.where(hits[other], gates[other : other + 1, :], 0.0) for other in range(members)], axis=0
        )
        coarse = scaled.astype(jnp.bfloat16)
        mix_weights[block, :, :row_count] = coarse
        mix_weights[block, :, row_count:] = (scaled - coarse.astype(jnp.float32)).astype(jnp.bfloat16)
        return picked.astype(jnp.bfloat16)

    def dispatch(step):
        block = steps[step]
        if step > 0:
            pass_up(block).wait_recv()
            forward(block)
        picked = place(block)
        for first in range(0, width, column):
            part = jnp.dot(
                picked, blocks[block, :, first : first + column], preferred_element_type=jnp.float32
            )
            for other in range(members):
                sent[block, other, :, first : first + column] = part[
                    other * capacity : (other + 1) * capacity
                ].astype(jnp.bfloat16)
        each_other(lambda other: deal(block, other).start())
        arrived[block, me] = sent[block, me]

    def gather_rows(buffer, block):
        for other in range(members):
            wide[other * capacity : (other + 1) * capacity] = buffer[block, other].astype(jnp.float32)

    def apply_expert(step):
        block = steps[step]
        each_other(lambda other: landing(arrived, arrived_sem, block, other).wait_recv())
        gather_rows(arrived, block)
        rows = wide[...].astype(jnp.bfloat16)
        gate = jnp.dot(rows, gate_w[...], preferred_element_type=jnp.float32)
        up = jnp.dot(rows, up_w[...], preferred_element_type=jnp.float32)
        hidden = (jax.nn.silu(gate) * up).astype(jnp.bfloat16)
        for first in range(0, width, column):
            part = jnp.dot(
                hidden, down_w[:, first : first + column], preferred_element_type=jnp.float32
            )
            for other in range(members):
                replies[block, other, :, first : first + column] = part[
                    other * capacity : (other + 1) * capacity
                ].astype(jnp.bfloat16)
        each_other(lambda other: reply(block, other).start())
        returned[block, me] = replies[block, me]

    def combine(step):
        block = steps[step]
        each_other(lambda other: landing(returned, returned_sem, block, other).wait_recv())
        gather_rows(returned, block)
        weights = mix_weights[block]
        for first in range(0, width, column):
            rows = wide[:, first : first + column].astype(jnp.bfloat16)
            both = lax.dot_general(
                weights, rows, (((0,), (0,)), ((), ())), preferred_element_type=jnp.float32
            )
            added = both[:row_count] + both[row_count:]
            if step == 0:
                total[:, first : first + column] += added
            else:
                partial[block, :, first : first + column] = added.astype(jnp.bfloat16)
        if step > 0:
            homeward(block).start()

    def shared():
        for load in loads[:3]:
            load.wait()
        rows = hidden_ref[...]
        gate = jnp.dot(rows, sgate_w[...], preferred_element_type=jnp.float32)
        up = jnp.dot(rows, sup_w[...], preferred_element_type=jnp.float32)
        hidden = (jax.nn.silu(gate) * up).astype(jnp.bfloat16)
        for first in range(0, width, column):
            total[:, first : first + column] = stream_ref[:, first : first + column] + jnp.dot(
                hidden, sdown_w[:, first : first + column], preferred_element_type=jnp.float32
            )

    pl.semaphore_wait(barrier, members - 1 + planes - 1)
    forward(plane)
    dispatch(0)
    shared()
    for load in loads[3:]:
        load.wait()
    apply_expert(0)
    for step in range(1, min(3, planes)):
        dispatch(step)
    for step in range(1, planes):
        apply_expert(step)
        combine(step - 1)
        if step + 2 < planes:
            dispatch(step + 2)
    combine(planes - 1)
    result = total[...]
    for step in range(1, planes):
        block = steps[step]
        pltpu.make_async_remote_copy(
            src_ref=partial.at[block],
            dst_ref=homed.at[block],
            send_sem=partial_sem.at[block],
            recv_sem=homed_sem.at[block],
            device_id=plane_id(block),
            device_id_type=MESH,
        ).wait_recv()
        result = result + homed[block].astype(jnp.float32)
    out_ref[...] = result.astype(out_ref.dtype)

    for step in range(planes):
        block = steps[step]

        @pl.when(goes_up(block))
        def _():
            pass_up(block).wait_send()

        @pl.when(goes_down(block))
        def _():
            pass_down(block).wait_send()

        each_other(lambda other: deal(block, other).wait_send())
        each_other(lambda other: reply(block, other).wait_send())
        if step > 0:
            homeward(block).wait_send()


def moe(routes, hidden, stream, weights, capacity, collective_id):
    sp_count, tp_count = lax.axis_size("sp"), lax.axis_size("tp")
    planes = planes_of(sp_count)
    members = sp_count * tp_count // planes
    rows, width = hidden.shape
    hidden_width = weights[0].shape[-1]
    capacity = -(-capacity // 8) * 8
    vmem = pl.BlockSpec(memory_space=pltpu.VMEM)
    pieces = pltpu.VMEM((planes, members, capacity, width), jnp.bfloat16)
    whole = pltpu.VMEM((planes, rows, width), jnp.bfloat16)
    pair = pltpu.SemaphoreType.DMA((planes, members))
    single = pltpu.SemaphoreType.DMA((planes,))
    inner = pltpu.VMEM((width, hidden_width), jnp.bfloat16)
    outer = pltpu.VMEM((hidden_width, width), jnp.bfloat16)
    return pl.pallas_call(
        functools.partial(moe_kernel, sp_count, tp_count, capacity),
        out_shape=jax.ShapeDtypeStruct((rows, width), jnp.bfloat16),
        in_specs=[vmem] * 3 + [pl.BlockSpec(memory_space=pl.ANY)] * 6,
        out_specs=vmem,
        scratch_shapes=[
            whole,
            pieces,
            pieces,
            pieces,
            pieces,
            whole,
            whole,
            pltpu.VMEM((planes, members * capacity, 2 * rows), jnp.bfloat16),
            pltpu.VMEM((members * capacity, width), jnp.float32),
            pltpu.VMEM((rows, width), jnp.float32),
            inner,
            inner,
            outer,
            inner,
            inner,
            outer,
            pltpu.SemaphoreType.DMA((6,)),
            pltpu.SemaphoreType.DMA,
            single,
            single,
            single,
            pair,
            pair,
            pair,
            pair,
            single,
            single,
        ],
        compiler_params=pltpu.CompilerParams(
            collective_id=collective_id, has_side_effects=True, vmem_limit_bytes=60 * 2**20
        ),
    )(routes, hidden, stream, *weights)


CHUNK = 16


def times(a, b):
    return (a[0] * b[0] - a[1] * b[1], a[0] * b[1] + a[1] * b[0])


def mixer(inputs, decay_real, decay_imag, log_step, input_re, input_im, output_re, output_im, skip, routes):
    length = inputs.shape[0]
    groups, states, channels = input_re.shape
    chunks = length // CHUNK
    step_size = jnp.exp(log_step)[:, None]
    log_rate = decay_real * step_size
    turn_angle = decay_imag * step_size

    def powers(count):
        magnitude = jnp.exp(count * log_rate)
        return (magnitude * jnp.cos(count * turn_angle), magnitude * jnp.sin(count * turn_angle))

    bar_re, bar_im = powers(1.0)
    denominator = decay_real * decay_real + decay_imag * decay_imag
    less_one = bar_re - 1.0
    coef = (
        (less_one * decay_real + bar_im * decay_imag) / denominator,
        (bar_im * decay_real - less_one * decay_imag) / denominator,
    )
    drive = times((coef[0][:, :, None], coef[1][:, :, None]), (input_re, input_im))
    steps = jnp.arange(1, CHUNK + 1, dtype=jnp.float32)
    ahead = powers(steps[:, None, None])
    ahead = tuple(jnp.swapaxes(part, 0, 1)[:, :, None, :] for part in ahead)
    reads = times(ahead, (output_re[:, None], output_im[:, None]))
    reads = jnp.concatenate([reads[0], -reads[1]], axis=3).reshape(
        groups, CHUNK * channels, 2 * states
    )
    back = powers(-steps[:, None, None])
    back = tuple(jnp.swapaxes(part, 0, 1)[:, :, None, :] for part in back)
    drive = tuple(jnp.swapaxes(part, 1, 2)[:, None] for part in drive)
    feeds = times(back, drive)
    feeds = jnp.concatenate(feeds, axis=3).reshape(groups, CHUNK * channels, 2 * states)
    rows = jnp.arange(CHUNK * channels, dtype=jnp.int32) // channels
    kernel = jnp.einsum("gsn,gtn->gst", feeds, reads, precision=HIGHEST)
    kernel = jnp.where(rows[:, None] <= rows[None, :], kernel, 0.0)
    wide = (
        inputs.reshape(chunks, CHUNK, groups, channels)
        .transpose(2, 0, 1, 3)
        .reshape(groups, chunks, CHUNK * channels)
        .astype(jnp.float32)
    )
    local = jnp.einsum("gks,gst->gkt", wide, kernel, precision=HIGHEST)
    driven = jnp.einsum("gks,gsn->gkn", wide, feeds, precision=HIGHEST)
    whole = tuple(part[:, None] for part in powers(float(CHUNK)))
    state = times(whole, (driven[:, :, :states], driven[:, :, states:]))
    offset = 1
    while offset < chunks:
        prior = tuple(
            jnp.pad(part[:, :-offset], ((0, 0), (offset, 0), (0, 0))) for part in state
        )
        moved = times(tuple(part[:, None] for part in powers(float(CHUNK * offset))), prior)
        state = (state[0] + moved[0], state[1] + moved[1])
        offset *= 2
    ends = jnp.concatenate([state[0][:, -1], state[1][:, -1]], axis=1)
    ends = ends.reshape(groups * states * 2 // 128, 128)
    gathered = gather_sp(jnp.concatenate([ends, routes], axis=0))
    pieces = gathered[:, : ends.shape[0]].reshape(-1, groups, 2 * states)
    all_routes = gathered[:, ends.shape[0] :]
    my_index = lax.axis_index("sp")
    sources = jnp.arange(pieces.shape[0], dtype=jnp.int32)
    earlier = sources < my_index
    distance = jnp.where(earlier, my_index - 1 - sources, 0).astype(jnp.float32)[:, None, None]
    weight = jnp.where(earlier, 1.0, 0.0).astype(jnp.float32)[:, None, None]
    block_angle = jnp.mod(float(length) * turn_angle, 2.0 * math.pi)
    magnitude = jnp.exp(distance * (float(length) * log_rate)) * weight
    factor = (
        magnitude * jnp.cos(distance * block_angle),
        magnitude * jnp.sin(distance * block_angle),
    )
    added = times(factor, (pieces[:, :, :states], pieces[:, :, states:]))
    carried = tuple(jnp.sum(part, axis=0)[:, None] for part in added)
    starts = powers(float(CHUNK) * jnp.arange(chunks, dtype=jnp.float32)[:, None, None])
    starts = tuple(jnp.swapaxes(part, 0, 1) for part in starts)
    carried = times(starts, carried)
    before = jnp.concatenate(
        [
            jnp.pad(state[i][:, :-1], ((0, 0), (1, 0), (0, 0))) + carried[i]
            for i in range(2)
        ],
        axis=2,
    )
    readout = local + jnp.einsum("gkn,gtn->gkt", before, reads, precision=HIGHEST)
    gains = jnp.broadcast_to(skip[:, None, :], (groups, CHUNK, channels))
    mixed = jax.nn.gelu(readout + gains.reshape(groups, 1, -1) * wide).astype(jnp.bfloat16)
    mixed = (
        mixed.reshape(groups, chunks, CHUNK, channels)
        .transpose(1, 2, 0, 3)
        .reshape(length, groups * channels)
    )
    return mixed, all_routes


def rms_scale(values, gain):
    return values * lax.rsqrt(jnp.mean(values * values, axis=-1, keepdims=True) + NORM_EPS) * gain


def on_device(
    mixer_input,
    residual,
    decay_real,
    decay_imag,
    log_step,
    input_re,
    input_im,
    output_re,
    output_im,
    skip_gain,
    glu_weight,
    glu_bias,
    mix_gain,
    out_weight,
    norm_gain,
    route_ids,
    route_gates,
    expert_gate,
    expert_up,
    expert_down,
    shared_gate,
    shared_up,
    shared_down,
):
    routes = jnp.concatenate([route_ids.astype(jnp.float32), route_gates], axis=1).T
    mixed, routes = mixer(
        mixer_input,
        decay_real,
        decay_imag,
        log_step,
        input_re,
        input_im,
        output_re,
        output_im,
        skip_gain,
        routes,
    )
    tp_count = lax.axis_size("tp")
    token_rows = exchange_tp(mixed.reshape(tp_count, -1, mixed.shape[1]))
    token_rows = token_rows.transpose(1, 0, 2).reshape(token_rows.shape[1], -1)
    pre_gate = jnp.dot(token_rows, glu_weight, preferred_element_type=jnp.float32) + glu_bias
    gated = token_rows.astype(jnp.float32) * jax.nn.sigmoid(pre_gate)
    normed = rms_scale(gated, mix_gain).astype(jnp.bfloat16)
    stream = residual.astype(jnp.float32) + jnp.dot(
        normed, out_weight, preferred_element_type=jnp.float32
    )
    hidden_in = rms_scale(stream, norm_gain).astype(jnp.bfloat16)
    row_count, top_count = route_ids.shape
    expert_count = lax.axis_size(("sp", "tp"))
    capacity = max(2, 3 * row_count * top_count // (2 * expert_count))
    weights = (expert_gate, expert_up, expert_down, shared_gate, shared_up, shared_down)
    return moe(routes, hidden_in, stream, weights, capacity, 3)


def solution(mesh):
    return jax.shard_map(
        on_device,
        mesh=mesh,
        in_specs=(
            P("sp", "tp"),
            P(("sp", "tp"), None),
            P("tp", None),
            P("tp", None),
            P("tp"),
            P("tp", None, None),
            P("tp", None, None),
            P("tp", None, None),
            P("tp", None, None),
            P("tp", None),
            P(),
            P(),
            P(),
            P(),
            P(),
            P(("sp", "tp"), None),
            P(("sp", "tp"), None),
            P(("sp", "tp"), None, None),
            P(("sp", "tp"), None, None),
            P(("sp", "tp"), None, None),
            P(),
            P(),
            P(),
        ),
        out_specs=P(("sp", "tp"), None),
        check_vma=False,
    )
```

```python
import functools
import math

import jax
import jax.numpy as jnp
from jax import lax
from jax.experimental import pallas as pl
from jax.experimental.pallas import tpu as pltpu
from jax.sharding import PartitionSpec as P

NORM_EPS = 1e-06
HIGHEST = lax.Precision.HIGHEST
MESH = pl.DeviceIdType.MESH


def times(a, b):
    return (a[0] * b[0] - a[1] * b[1], a[0] * b[1] + a[1] * b[0])


def rms_scale(values, gain):
    return values * lax.rsqrt(jnp.mean(values * values, axis=-1, keepdims=True) + NORM_EPS) * gain


def flatten_rows(values, count):
    groups, states = values.shape
    width = groups * states
    lanes = lax.broadcasted_iota(jnp.int32, (states, width), 1)
    spread = jnp.where(
        jnp.bitwise_and(lanes, states - 1) == lax.broadcasted_iota(jnp.int32, (states, width), 0), 1.0, 0.0
    )
    tiled = jnp.dot(values, spread, precision=HIGHEST, preferred_element_type=jnp.float32)
    first = lax.broadcasted_iota(jnp.int32, (groups, width), 0) * states
    lanes = lax.broadcasted_iota(jnp.int32, (groups, width), 1)
    own = jnp.logical_and(lanes >= first, lanes < first + states)
    row = jnp.sum(jnp.where(own, tiled, 0.0), axis=0, keepdims=True)
    return jnp.broadcast_to(row, (count, width))


def split_in_two(values):
    coarse = values.astype(jnp.bfloat16)
    return coarse, (values - coarse.astype(jnp.float32)).astype(jnp.bfloat16)


def front_kernel(
    sp_count,
    tp_count,
    inputs_ref,
    residual_ref,
    real_ref,
    imag_ref,
    step_ref,
    in_re_ref,
    in_im_ref,
    out_re_ref,
    out_im_ref,
    skip_ref,
    routes_ref,
    glu_hbm,
    bias_ref,
    mix_gain_ref,
    proj_hbm,
    norm_gain_ref,
    hidden_ref,
    stream_ref,
    all_routes_ref,
    feeds,
    reads,
    states_ref,
    permuted,
    mixed_ref,
    end_ref,
    ends,
    tokens,
    glu_w,
    proj_w,
    weight_sem,
    end_send,
    end_recv,
    route_send,
    route_recv,
    token_send,
    token_recv,
):
    sp = lax.axis_index("sp")
    tp = lax.axis_index("tp")
    length, channel_count = inputs_ref.shape
    groups, states, channels = in_re_ref.shape
    wide = groups * states
    segment = length // 8
    rows = length // tp_count

    barrier = pltpu.get_barrier_semaphore()

    def greet_sp(step, carry):
        pl.semaphore_signal(
            barrier, inc=1, device_id=(lax.rem(sp + step, sp_count), tp), device_id_type=MESH
        )
        return carry

    def greet_tp(step, carry):
        pl.semaphore_signal(
            barrier, inc=1, device_id=(sp, lax.rem(tp + step, tp_count)), device_id_type=MESH
        )
        return carry

    lax.fori_loop(1, sp_count, greet_sp, 0)
    lax.fori_loop(1, tp_count, greet_tp, 0)
    loads = [
        pltpu.make_async_copy(glu_hbm, glu_w, weight_sem.at[0]),
        pltpu.make_async_copy(proj_hbm, proj_w, weight_sem.at[1]),
    ]
    for load in loads:
        load.start()

    def end_to(other):
        return pltpu.make_async_remote_copy(
            src_ref=end_ref,
            dst_ref=ends.at[sp],
            send_sem=end_send.at[other],
            recv_sem=end_recv.at[sp],
            device_id=(other, tp),
            device_id_type=MESH,
        )

    def end_from(other):
        return pltpu.make_async_remote_copy(
            src_ref=end_ref,
            dst_ref=ends.at[other],
            send_sem=end_send.at[other],
            recv_sem=end_recv.at[other],
            device_id=(other, tp),
            device_id_type=MESH,
        )

    def route_to(other):
        return pltpu.make_async_remote_copy(
            src_ref=routes_ref,
            dst_ref=all_routes_ref.at[sp],
            send_sem=route_send.at[other],
            recv_sem=route_recv.at[sp],
            device_id=(other, tp),
            device_id_type=MESH,
        )

    def route_from(other):
        return pltpu.make_async_remote_copy(
            src_ref=routes_ref,
            dst_ref=all_routes_ref.at[other],
            send_sem=route_send.at[other],
            recv_sem=route_recv.at[other],
            device_id=(other, tp),
            device_id_type=MESH,
        )

    def token_to(other):
        return pltpu.make_async_remote_copy(
            src_ref=mixed_ref.at[other],
            dst_ref=tokens.at[tp],
            send_sem=token_send.at[other],
            recv_sem=token_recv.at[tp],
            device_id=(sp, other),
            device_id_type=MESH,
        )

    def token_from(other):
        return pltpu.make_async_remote_copy(
            src_ref=mixed_ref.at[other],
            dst_ref=tokens.at[other],
            send_sem=token_send.at[other],
            recv_sem=token_recv.at[other],
            device_id=(sp, other),
            device_id_type=MESH,
        )

    def each_sp(action):
        def body(step, carry):
            action(lax.rem(sp + step, sp_count))
            return carry

        lax.fori_loop(1, sp_count, body, 0)

    def each_tp(action):
        def body(step, carry):
            action(lax.rem(tp + step, tp_count))
            return carry

        lax.fori_loop(1, tp_count, body, 0)

    decay_real = flatten_rows(real_ref[...], 8)
    decay_imag = flatten_rows(imag_ref[...], 8)
    own_first = lax.broadcasted_iota(jnp.int32, (groups, wide), 0) * states
    own_lane = lax.broadcasted_iota(jnp.int32, (groups, wide), 1)
    own_group = jnp.where(
        jnp.logical_and(own_lane >= own_first, own_lane < own_first + states), 1.0, 0.0
    )
    step_size = jnp.exp(
        jnp.dot(
            jnp.broadcast_to(step_ref[...], (8, groups)),
            own_group,
            precision=HIGHEST,
            preferred_element_type=jnp.float32,
        )
    )
    magnitude = jnp.exp(decay_real * step_size)
    bar = (magnitude * jnp.cos(decay_imag * step_size), magnitude * jnp.sin(decay_imag * step_size))
    denominator = decay_real * decay_real + decay_imag * decay_imag
    less_one = bar[0] - 1.0
    coef = (
        (less_one * decay_real + bar[1] * decay_imag) / denominator,
        (bar[1] * decay_real - less_one * decay_imag) / denominator,
    )
    identity = jnp.where(
        lax.broadcasted_iota(jnp.int32, (channels, channels), 0)
        == lax.broadcasted_iota(jnp.int32, (channels, channels), 1),
        1.0,
        0.0,
    )
    maps = tuple(
        lax.dot_general(
            identity,
            ref[...].reshape(wide, channels),
            (((1,), (1,)), ((), ())),
            precision=HIGHEST,
            preferred_element_type=jnp.float32,
        )
        for ref in (in_re_ref, in_im_ref)
    )
    drive = times((coef[0][:1], coef[1][:1]), maps)
    lane = lax.broadcasted_iota(jnp.int32, (channels, wide), 1)
    for part in range(2):
        for index, piece in enumerate(split_in_two(drive[part])):
            piece = piece.astype(jnp.float32)
            for group in range(groups):
                own = jnp.logical_and(lane >= group * states, lane < (group + 1) * states)
                feeds[
                    index * channel_count + group * channels : index * channel_count + (group + 1) * channels,
                    part * wide : (part + 1) * wide,
                ] = jnp.where(own, piece, 0.0).astype(jnp.bfloat16)
    spread = jnp.where(
        jnp.bitwise_and(lax.broadcasted_iota(jnp.int32, (states, wide), 1), states - 1)
        == lax.broadcasted_iota(jnp.int32, (states, wide), 0),
        1.0,
        0.0,
    ).astype(jnp.bfloat16)
    for part, ref in enumerate((out_re_ref, out_im_ref)):
        table = ref[...].reshape(channel_count, states)
        table = table if part == 0 else -table
        for index, piece in enumerate(split_in_two(table)):
            tiled = jnp.dot(piece, spread, preferred_element_type=jnp.float32)
            for group in range(groups):
                own = jnp.logical_and(lane >= group * states, lane < (group + 1) * states)
                reads[
                    index,
                    group * channels : (group + 1) * channels,
                    part * wide : (part + 1) * wide,
                ] = jnp.where(own, tiled[group * channels : (group + 1) * channels], 0.0).astype(jnp.bfloat16)

    order = lax.broadcasted_iota(jnp.int32, (length, length), 0)
    shuffle = jnp.where(
        lax.broadcasted_iota(jnp.int32, (length, length), 1)
        == jnp.bitwise_and(order, 7) * segment + lax.shift_right_logical(order, 3),
        1.0,
        0.0,
    ).astype(jnp.bfloat16)
    permuted[...] = jnp.dot(shuffle, inputs_ref[...], preferred_element_type=jnp.float32).astype(jnp.bfloat16)
    block = min(512, wide)
    for first in range(0, 2 * wide, block):
        states_ref[:, first : first + block] = jnp.dot(
            permuted[...], feeds[:channel_count, first : first + block], preferred_element_type=jnp.float32
        ) + jnp.dot(
            permuted[...], feeds[channel_count:, first : first + block], preferred_element_type=jnp.float32
        )

    def advance(start, keep):
        def body(index, state):
            at = pl.ds(pl.multiple_of(index * 8, 8), 8)
            moved = times(bar, state)
            state = (moved[0] + states_ref[at, :wide], moved[1] + states_ref[at, wide:])
            if keep:
                states_ref[at, :wide] = state[0]
                states_ref[at, wide:] = state[1]
            return state

        return lax.fori_loop(0, segment, body, start, unroll=4)

    zero = jnp.zeros((8, wide), jnp.float32)
    tails = advance((zero, zero), False)
    row = tuple(part[:1] for part in bar)
    power = 1
    while power < segment:
        row = times(row, row)
        power *= 2
    over_segment = row
    while power < length:
        row = times(row, row)
        power *= 2
    over_block = row
    nothing = (zero[:1], zero[:1])
    total = nothing
    for index in range(8):
        moved = times(over_segment, total)
        total = tuple(moved[part] + tails[part][index : index + 1] for part in range(2))
    end_ref[0:1] = total[0]
    end_ref[1:2] = total[1]
    pl.semaphore_wait(barrier, sp_count - 1 + tp_count - 1)
    each_sp(lambda other: end_to(other).start())
    each_sp(lambda other: route_to(other).start())
    all_routes_ref[sp] = routes_ref[...]
    each_sp(lambda other: end_from(other).wait_recv())
    carried = nothing
    for source in range(sp_count):
        moved = times(over_block, carried)
        earlier = sp > source
        carried = tuple(
            jnp.where(earlier, moved[part] + ends[source, part : part + 1], carried[part]) for part in range(2)
        )
    begins = ([], [])
    for index in range(8):
        for part in range(2):
            begins[part].append(carried[part])
        moved = times(over_segment, carried)
        carried = tuple(moved[part] + tails[part][index : index + 1] for part in range(2))
    advance(tuple(jnp.concatenate(part, axis=0) for part in begins), True)

    gains = flatten_rows(skip_ref[...], 1)
    across = (((1,), (1,)), ((), ()))
    mixed = []
    for first in range(0, length, rows):
        coarse, fine = split_in_two(states_ref[first : first + rows])
        readout = (
            lax.dot_general(coarse, reads[0], across, preferred_element_type=jnp.float32)
            + lax.dot_general(fine, reads[0], across, preferred_element_type=jnp.float32)
            + lax.dot_general(coarse, reads[1], across, preferred_element_type=jnp.float32)
        )
        direct = gains * permuted[first : first + rows].astype(jnp.float32)
        mixed.append(jax.nn.gelu(readout + direct).astype(jnp.bfloat16))
    mixed = jnp.concatenate(mixed, axis=0)
    ordered = lax.dot_general(
        shuffle, mixed, (((0,), (0,)), ((), ())), preferred_element_type=jnp.float32
    ).astype(jnp.bfloat16)
    for other in range(tp_count):
        mixed_ref[other] = ordered[other * rows : (other + 1) * rows]
    each_tp(lambda other: token_to(other).start())
    tokens[tp] = mixed_ref[tp]
    for load in loads:
        load.wait()
    each_tp(lambda other: token_from(other).wait_recv())
    token_rows = jnp.concatenate([tokens[other] for other in range(tp_count)], axis=1)
    pre_gate = jnp.dot(token_rows, glu_w[...], preferred_element_type=jnp.float32) + bias_ref[...]
    gated = token_rows.astype(jnp.float32) * jax.nn.sigmoid(pre_gate)
    normed = rms_scale(gated, mix_gain_ref[...]).astype(jnp.bfloat16)
    stream = residual_ref[...].astype(jnp.float32) + jnp.dot(
        normed, proj_w[...], preferred_element_type=jnp.float32
    )
    stream_ref[...] = stream
    hidden_ref[...] = rms_scale(stream, norm_gain_ref[...]).astype(jnp.bfloat16)
    each_sp(lambda other: route_from(other).wait_recv())
    each_sp(lambda other: end_to(other).wait_send())
    each_sp(lambda other: route_to(other).wait_send())
    each_tp(lambda other: token_to(other).wait_send())


def front(
    mixer_input,
    residual,
    decay_real,
    decay_imag,
    log_step,
    input_re,
    input_im,
    output_re,
    output_im,
    skip_gain,
    routes,
    glu_weight,
    glu_bias,
    mix_gain,
    out_weight,
    norm_gain,
    collective_id,
):
    sp_count, tp_count = lax.axis_size("sp"), lax.axis_size("tp")
    length, channel_count = mixer_input.shape
    groups, states, channels = input_re.shape
    rows, width = residual.shape
    wide = groups * states
    vmem = pl.BlockSpec(memory_space=pltpu.VMEM)
    hbm = pl.BlockSpec(memory_space=pl.ANY)
    dma = pltpu.SemaphoreType.DMA
    return pl.pallas_call(
        functools.partial(front_kernel, sp_count, tp_count),
        out_shape=(
            jax.ShapeDtypeStruct((rows, width), jnp.bfloat16),
            jax.ShapeDtypeStruct((rows, width), jnp.float32),
            jax.ShapeDtypeStruct((sp_count,) + routes.shape, jnp.float32),
        ),
        in_specs=[vmem] * 11 + [hbm, vmem, vmem, hbm, vmem],
        out_specs=(vmem, vmem, vmem),
        scratch_shapes=[
            pltpu.VMEM((2 * channel_count, 2 * wide), jnp.bfloat16),
            pltpu.VMEM((2, channel_count, 2 * wide), jnp.bfloat16),
            pltpu.VMEM((length, 2 * wide), jnp.float32),
            pltpu.VMEM((length, channel_count), jnp.bfloat16),
            pltpu.VMEM((tp_count, rows, channel_count), jnp.bfloat16),
            pltpu.VMEM((2, wide), jnp.float32),
            pltpu.VMEM((sp_count, 2, wide), jnp.float32),
            pltpu.VMEM((tp_count, rows, channel_count), jnp.bfloat16),
            pltpu.VMEM(glu_weight.shape, jnp.bfloat16),
            pltpu.VMEM(out_weight.shape, jnp.bfloat16),
            dma((2,)),
            dma((sp_count,)),
            dma((sp_count,)),
            dma((sp_count,)),
            dma((sp_count,)),
            dma((tp_count,)),
            dma((tp_count,)),
        ],
        compiler_params=pltpu.CompilerParams(
            collective_id=collective_id, has_side_effects=True, vmem_limit_bytes=48 * 2**20
        ),
    )(
        mixer_input,
        residual,
        decay_real,
        decay_imag,
        log_step[None, :],
        input_re,
        input_im,
        output_re,
        output_im,
        skip_gain,
        routes,
        glu_weight,
        glu_bias[None, :],
        mix_gain[None, :],
        out_weight,
        norm_gain[None, :],
    )


def planes_of(sp_count):
    return math.gcd(sp_count, 4)


def visiting_order(planes):
    return [sorted(range(planes), key=lambda other: (abs(other - own), -other)) for own in range(planes)]


def moe_kernel(
    sp_count,
    tp_count,
    capacity,
    routes_ref,
    hidden_ref,
    stream_ref,
    gate_hbm,
    up_hbm,
    down_hbm,
    sgate_hbm,
    sup_hbm,
    sdown_hbm,
    out_ref,
    blocks,
    sent,
    arrived,
    replies,
    returned,
    partial,
    homed,
    mix_weights,
    wide,
    total,
    gate_w,
    up_w,
    down_w,
    sgate_w,
    sup_w,
    sdown_w,
    weight_sem,
    own_sem,
    up_sem,
    down_sem,
    block_sem,
    sent_sem,
    arrived_sem,
    replies_sem,
    returned_sem,
    partial_sem,
    homed_sem,
):
    planes = planes_of(sp_count)
    rows_y = sp_count // planes
    members = rows_y * tp_count
    row_count, width = hidden_ref.shape
    hidden_width = gate_w.shape[1]
    slots = members * capacity
    top_count = routes_ref.shape[1] // 2
    column = min(512, width)
    sp = lax.axis_index("sp")
    tp = lax.axis_index("tp")
    plane = sp // rows_y
    row_y = lax.rem(sp, rows_y)
    me = row_y * tp_count + tp

    def member_id(other):
        return (plane * rows_y + other // tp_count, lax.rem(other, tp_count))

    def plane_id(other):
        return (other * rows_y + row_y, tp)

    loads = [
        pltpu.make_async_copy(source.at[0] if len(source.shape) == 3 else source, target, weight_sem.at[number])
        for number, (source, target) in enumerate(
            (
                (sgate_hbm, sgate_w),
                (sup_hbm, sup_w),
                (sdown_hbm, sdown_w),
                (gate_hbm, gate_w),
                (up_hbm, up_w),
                (down_hbm, down_w),
            )
        )
    ]
    barrier = pltpu.get_barrier_semaphore()

    def greet_member(step, carry):
        pl.semaphore_signal(
            barrier, inc=1, device_id=member_id(lax.rem(me + step, members)), device_id_type=MESH
        )
        return carry

    def greet_plane(step, carry):
        pl.semaphore_signal(
            barrier, inc=1, device_id=plane_id(lax.rem(plane + step, planes)), device_id_type=MESH
        )
        return carry

    lax.fori_loop(1, members, greet_member, 0)
    lax.fori_loop(1, planes, greet_plane, 0)
    for load in loads:
        load.start()
    blocks[plane] = hidden_ref[...]

    order = visiting_order(planes)

    def visited(step):
        block = jnp.int32(order[0][step])
        for own in range(1, planes):
            block = jnp.where(plane == own, order[own][step], block)
        return block

    steps = [plane] + [visited(step) for step in range(1, planes)]

    def pass_up(block):
        return pltpu.make_async_remote_copy(
            src_ref=blocks.at[block],
            dst_ref=blocks.at[block],
            send_sem=up_sem.at[block],
            recv_sem=block_sem.at[block],
            device_id=plane_id(jnp.minimum(plane + 1, planes - 1)),
            device_id_type=MESH,
        )

    def pass_down(block):
        return pltpu.make_async_remote_copy(
            src_ref=blocks.at[block],
            dst_ref=blocks.at[block],
            send_sem=down_sem.at[block],
            recv_sem=block_sem.at[block],
            device_id=plane_id(jnp.maximum(plane - 1, 0)),
            device_id_type=MESH,
        )

    def goes_up(block):
        return jnp.logical_and(block <= plane, plane < planes - 1)

    def goes_down(block):
        return jnp.logical_and(block >= plane, plane > 0)

    def forward(block):
        @pl.when(goes_up(block))
        def _():
            pass_up(block).start()

        @pl.when(goes_down(block))
        def _():
            pass_down(block).start()

    def deal(block, other):
        return pltpu.make_async_remote_copy(
            src_ref=sent.at[block, other],
            dst_ref=arrived.at[block, me],
            send_sem=sent_sem.at[block, other],
            recv_sem=arrived_sem.at[block, me],
            device_id=member_id(other),
            device_id_type=MESH,
        )

    def reply(block, other):
        return pltpu.make_async_remote_copy(
            src_ref=replies.at[block, other],
            dst_ref=returned.at[block, me],
            send_sem=replies_sem.at[block, other],
            recv_sem=returned_sem.at[block, me],
            device_id=member_id(other),
            device_id_type=MESH,
        )

    def landing(buffer, sem, block, other):
        return pltpu.make_async_remote_copy(
            src_ref=buffer.at[block, other],
            dst_ref=buffer.at[block, other],
            send_sem=sent_sem.at[block, other],
            recv_sem=sem.at[block, other],
            device_id=member_id(other),
            device_id_type=MESH,
        )

    def homeward(block):
        return pltpu.make_async_remote_copy(
            src_ref=partial.at[block],
            dst_ref=homed.at[plane],
            send_sem=partial_sem.at[block],
            recv_sem=homed_sem.at[plane],
            device_id=plane_id(block),
            device_id_type=MESH,
        )

    def each_other(action):
        def body(step, carry):
            action(lax.rem(me + step, members))
            return carry

        lax.fori_loop(1, members, body, 0)

    def place(block):
        routes = routes_ref[block * rows_y + row_y]
        experts = (lax.broadcasted_iota(jnp.int32, (members, row_count), 0) + plane * members).astype(
            jnp.float32
        )
        named = jnp.zeros((members, row_count), jnp.float32)
        gates = jnp.zeros((members, row_count), jnp.float32)
        for index in range(top_count):
            hit = experts == routes[index : index + 1, :]
            named = named + jnp.where(hit, 1.0, 0.0)
            gates = gates + jnp.where(hit, routes[top_count + index : top_count + index + 1, :], 0.0)
        before = (
            lax.broadcasted_iota(jnp.int32, (row_count, row_count), 0)
            < lax.broadcasted_iota(jnp.int32, (row_count, row_count), 1)
        )
        ranks = jnp.dot(
            named.astype(jnp.bfloat16),
            jnp.where(before, 1.0, 0.0).astype(jnp.bfloat16),
            preferred_element_type=jnp.float32,
        )
        ranks = jnp.where(named > 0.5, ranks, -1.0)
        numbers = lax.broadcasted_iota(jnp.int32, (capacity, row_count), 0).astype(jnp.float32)
        hits = [ranks[other : other + 1, :] == numbers for other in range(members)]
        picked = jnp.concatenate([jnp.where(hit, 1.0, 0.0) for hit in hits], axis=0)
        scaled = jnp.concatenate(
            [jnp.where(hits[other], gates[other : other + 1, :], 0.0) for other in range(members)], axis=0
        )
        coarse = scaled.astype(jnp.bfloat16)
        mix_weights[block, :, :row_count] = coarse
        mix_weights[block, :, row_count:] = (scaled - coarse.astype(jnp.float32)).astype(jnp.bfloat16)
        return picked.astype(jnp.bfloat16)

    def dispatch(step):
        block = steps[step]
        if step > 0:
            pass_up(block).wait_recv()
            forward(block)
        picked = place(block)
        for first in range(0, width, column):
            part = jnp.dot(
                picked, blocks[block, :, first : first + column], preferred_element_type=jnp.float32
            )
            for other in range(members):
                sent[block, other, :, first : first + column] = part[
                    other * capacity : (other + 1) * capacity
                ].astype(jnp.bfloat16)
        each_other(lambda other: deal(block, other).start())
        arrived[block, me] = sent[block, me]

    def gather_rows(buffer, block):
        for other in range(members):
            wide[other * capacity : (other + 1) * capacity] = buffer[block, other].astype(jnp.float32)

    def apply_expert(step):
        block = steps[step]
        each_other(lambda other: landing(arrived, arrived_sem, block, other).wait_recv())
        gather_rows(arrived, block)
        rows = wide[...].astype(jnp.bfloat16)
        gate = jnp.dot(rows, gate_w[...], preferred_element_type=jnp.float32)
        up = jnp.dot(rows, up_w[...], preferred_element_type=jnp.float32)
        hidden = (jax.nn.silu(gate) * up).astype(jnp.bfloat16)
        for first in range(0, width, column):
            part = jnp.dot(
                hidden, down_w[:, first : first + column], preferred_element_type=jnp.float32
            )
            for other in range(members):
                replies[block, other, :, first : first + column] = part[
                    other * capacity : (other + 1) * capacity
                ].astype(jnp.bfloat16)
        each_other(lambda other: reply(block, other).start())
        returned[block, me] = replies[block, me]

    def combine(step):
        block = steps[step]
        each_other(lambda other: landing(returned, returned_sem, block, other).wait_recv())
        gather_rows(returned, block)
        weights = mix_weights[block]
        for first in range(0, width, column):
            rows = wide[:, first : first + column].astype(jnp.bfloat16)
            both = lax.dot_general(
                weights, rows, (((0,), (0,)), ((), ())), preferred_element_type=jnp.float32
            )
            added = both[:row_count] + both[row_count:]
            if step == 0:
                total[:, first : first + column] += added
            else:
                partial[block, :, first : first + column] = added.astype(jnp.bfloat16)
        if step > 0:
            homeward(block).start()

    def shared():
        for load in loads[:3]:
            load.wait()
        rows = hidden_ref[...]
        gate = jnp.dot(rows, sgate_w[...], preferred_element_type=jnp.float32)
        up = jnp.dot(rows, sup_w[...], preferred_element_type=jnp.float32)
        hidden = (jax.nn.silu(gate) * up).astype(jnp.bfloat16)
        for first in range(0, width, column):
            total[:, first : first + column] = stream_ref[:, first : first + column] + jnp.dot(
                hidden, sdown_w[:, first : first + column], preferred_element_type=jnp.float32
            )

    pl.semaphore_wait(barrier, members - 1 + planes - 1)
    forward(plane)
    dispatch(0)
    shared()
    for load in loads[3:]:
        load.wait()
    apply_expert(0)
    for step in range(1, min(3, planes)):
        dispatch(step)
    for step in range(1, planes):
        apply_expert(step)
        combine(step - 1)
        if step + 2 < planes:
            dispatch(step + 2)
    combine(planes - 1)
    result = total[...]
    for step in range(1, planes):
        block = steps[step]
        pltpu.make_async_remote_copy(
            src_ref=partial.at[block],
            dst_ref=homed.at[block],
            send_sem=partial_sem.at[block],
            recv_sem=homed_sem.at[block],
            device_id=plane_id(block),
            device_id_type=MESH,
        ).wait_recv()
        result = result + homed[block].astype(jnp.float32)
    out_ref[...] = result.astype(out_ref.dtype)

    for step in range(planes):
        block = steps[step]

        @pl.when(goes_up(block))
        def _():
            pass_up(block).wait_send()

        @pl.when(goes_down(block))
        def _():
            pass_down(block).wait_send()

        each_other(lambda other: deal(block, other).wait_send())
        each_other(lambda other: reply(block, other).wait_send())
        if step > 0:
            homeward(block).wait_send()


def moe(routes, hidden, stream, weights, capacity, collective_id):
    sp_count, tp_count = lax.axis_size("sp"), lax.axis_size("tp")
    planes = planes_of(sp_count)
    members = sp_count * tp_count // planes
    rows, width = hidden.shape
    hidden_width = weights[0].shape[-1]
    capacity = -(-capacity // 8) * 8
    vmem = pl.BlockSpec(memory_space=pltpu.VMEM)
    pieces = pltpu.VMEM((planes, members, capacity, width), jnp.bfloat16)
    whole = pltpu.VMEM((planes, rows, width), jnp.bfloat16)
    pair = pltpu.SemaphoreType.DMA((planes, members))
    single = pltpu.SemaphoreType.DMA((planes,))
    inner = pltpu.VMEM((width, hidden_width), jnp.bfloat16)
    outer = pltpu.VMEM((hidden_width, width), jnp.bfloat16)
    return pl.pallas_call(
        functools.partial(moe_kernel, sp_count, tp_count, capacity),
        out_shape=jax.ShapeDtypeStruct((rows, width), jnp.bfloat16),
        in_specs=[vmem] * 3 + [pl.BlockSpec(memory_space=pl.ANY)] * 6,
        out_specs=vmem,
        scratch_shapes=[
            whole,
            pieces,
            pieces,
            pieces,
            pieces,
            whole,
            whole,
            pltpu.VMEM((planes, members * capacity, 2 * rows), jnp.bfloat16),
            pltpu.VMEM((members * capacity, width), jnp.float32),
            pltpu.VMEM((rows, width), jnp.float32),
            inner,
            inner,
            outer,
            inner,
            inner,
            outer,
            pltpu.SemaphoreType.DMA((6,)),
            pltpu.SemaphoreType.DMA,
            single,
            single,
            single,
            pair,
            pair,
            pair,
            pair,
            single,
            single,
        ],
        compiler_params=pltpu.CompilerParams(
            collective_id=collective_id, has_side_effects=True, vmem_limit_bytes=60 * 2**20
        ),
    )(routes, hidden, stream, *weights)


def on_device(
    mixer_input,
    residual,
    decay_real,
    decay_imag,
    log_step,
    input_re,
    input_im,
    output_re,
    output_im,
    skip_gain,
    glu_weight,
    glu_bias,
    mix_gain,
    out_weight,
    norm_gain,
    route_ids,
    route_gates,
    expert_gate,
    expert_up,
    expert_down,
    shared_gate,
    shared_up,
    shared_down,
):
    routes = jnp.concatenate([route_ids.astype(jnp.float32), route_gates], axis=1).T
    hidden_in, stream, routes = front(
        mixer_input,
        residual,
        decay_real,
        decay_imag,
        log_step,
        input_re,
        input_im,
        output_re,
        output_im,
        skip_gain,
        routes,
        glu_weight,
        glu_bias,
        mix_gain,
        out_weight,
        norm_gain,
        1,
    )
    row_count, top_count = route_ids.shape
    expert_count = lax.axis_size(("sp", "tp"))
    capacity = max(2, 3 * row_count * top_count // (2 * expert_count))
    weights = (expert_gate, expert_up, expert_down, shared_gate, shared_up, shared_down)
    return moe(routes, hidden_in, stream, weights, capacity, 2)


def solution(mesh):
    return jax.shard_map(
        on_device,
        mesh=mesh,
        in_specs=(
            P("sp", "tp"),
            P(("sp", "tp"), None),
            P("tp", None),
            P("tp", None),
            P("tp"),
            P("tp", None, None),
            P("tp", None, None),
            P("tp", None, None),
            P("tp", None, None),
            P("tp", None),
            P(),
            P(),
            P(),
            P(),
            P(),
            P(("sp", "tp"), None),
            P(("sp", "tp"), None),
            P(("sp", "tp"), None, None),
            P(("sp", "tp"), None, None),
            P(("sp", "tp"), None, None),
            P(),
            P(),
            P(),
        ),
        out_specs=P(("sp", "tp"), None),
        check_vma=False,
    )
```

```python
import functools
import math

import jax
import jax.numpy as jnp
from jax import lax
from jax.experimental import pallas as pl
from jax.experimental.pallas import tpu as pltpu
from jax.sharding import PartitionSpec as P

NORM_EPS = 1e-06
HIGHEST = lax.Precision.HIGHEST
MESH = pl.DeviceIdType.MESH


def times(a, b):
    return (a[0] * b[0] - a[1] * b[1], a[0] * b[1] + a[1] * b[0])


def rms_scale(values, gain):
    return values * lax.rsqrt(jnp.mean(values * values, axis=-1, keepdims=True) + NORM_EPS) * gain


def flatten_rows(values, count):
    groups, states = values.shape
    width = groups * states
    lanes = lax.broadcasted_iota(jnp.int32, (states, width), 1)
    spread = jnp.where(
        jnp.bitwise_and(lanes, states - 1) == lax.broadcasted_iota(jnp.int32, (states, width), 0), 1.0, 0.0
    )
    tiled = jnp.dot(values, spread, precision=HIGHEST, preferred_element_type=jnp.float32)
    first = lax.broadcasted_iota(jnp.int32, (groups, width), 0) * states
    lanes = lax.broadcasted_iota(jnp.int32, (groups, width), 1)
    own = jnp.logical_and(lanes >= first, lanes < first + states)
    row = jnp.sum(jnp.where(own, tiled, 0.0), axis=0, keepdims=True)
    return jnp.broadcast_to(row, (count, width))


def split_in_two(values):
    coarse = values.astype(jnp.bfloat16)
    return coarse, (values - coarse.astype(jnp.float32)).astype(jnp.bfloat16)


SPLIT = 2
SHARE = 4
STAGES = (
    "A00A01F10F20A20F21A21A10F11S00F30B20C20A11",
    "F31A30C21A31C22C23B10C10C11B30C12C13C30B00",
    "C31C32C00C33C01C02C03",
)


def stages_of(planes):
    if planes == 4:
        return [
            (text[at], int(text[at + 1]), int(text[at + 2])) for text in STAGES for at in range(0, len(text), 3)
        ]
    stages = [("A", 0, part) for part in range(SPLIT)] + [("S", 0, 0)]
    for step in range(1, planes):
        stages += [(stage, step, part) for part in range(SPLIT) for stage in "FA"]
        stages += [("B", step, 0)] + [("C", step, part) for part in range(SHARE)]
    return stages + [("B", 0, 0)] + [("C", 0, part) for part in range(SHARE)]


def planes_of(sp_count):
    return math.gcd(sp_count, 4)


def visiting_order(planes):
    return [sorted(range(planes), key=lambda other: (abs(other - own), -other)) for own in range(planes)]


def layer_kernel(
    sp_count,
    tp_count,
    capacity,
    *refs,
):
    sources = refs[:23]
    out_ref = refs[23]
    held = refs[24:47]
    (
        inputs_ref,
        residual_ref,
        real_ref,
        imag_ref,
        step_ref,
        in_re_ref,
        in_im_ref,
        out_re_ref,
        out_im_ref,
        skip_ref,
        ids_ref,
        gates_ref,
        glu_w,
        bias_ref,
        mix_gain_ref,
        proj_w,
        norm_gain_ref,
        sgate_w,
        sup_w,
        sdown_w,
        gate_w,
        up_w,
        down_w,
    ) = held
    (
        feeds,
        reads,
        states_ref,
        permuted,
        mixed_ref,
        end_ref,
        ends,
        tokens,
        routes_ref,
        all_routes,
        picks,
        hidden_ref,
        blocks,
        sent,
        arrived,
        replies,
        returned,
        partial,
        homed,
        mix_weights,
        wide_rows,
        total,
        load_sem,
        end_send,
        end_recv,
        route_send,
        route_recv,
        token_send,
        token_recv,
        up_sem,
        down_sem,
        block_sem,
        sent_sem,
        arrived_sem,
        replies_sem,
        returned_sem,
        partial_sem,
        homed_sem,
    ) = refs[47:]
    sp = lax.axis_index("sp")
    tp = lax.axis_index("tp")
    length, channel_count = inputs_ref.shape
    groups, channels, states = in_re_ref.shape
    wide = groups * states
    segment = length // 8
    rows = length // tp_count
    planes = planes_of(sp_count)
    rows_y = sp_count // planes
    members = rows_y * tp_count
    width = residual_ref.shape[1]
    row_count = rows
    top_count = ids_ref.shape[0]
    part_width = width // SPLIT
    share_width = width // SHARE
    column = min(512, part_width, share_width)
    plane = sp // rows_y
    row_y = lax.rem(sp, rows_y)
    me = row_y * tp_count + tp

    barrier = pltpu.get_barrier_semaphore()

    def greet_sp(step, carry):
        pl.semaphore_signal(
            barrier, inc=1, device_id=(lax.rem(sp + step, sp_count), tp), device_id_type=MESH
        )
        return carry

    def member_id(other):
        return (plane * rows_y + other // tp_count, lax.rem(other, tp_count))

    def plane_id(other):
        return (other * rows_y + row_y, tp)

    def greet_member(step, carry):
        pl.semaphore_signal(
            barrier, inc=1, device_id=member_id(lax.rem(me + step, members)), device_id_type=MESH
        )
        return carry

    loads = [
        pltpu.make_async_copy(source, target, load_sem.at[number])
        for number, (source, target) in enumerate(zip(sources, held))
    ]
    for load in loads:
        load.start()
    lax.fori_loop(1, sp_count, greet_sp, 0)
    lax.fori_loop(1, members, greet_member, 0)
    def end_to(other):
        return pltpu.make_async_remote_copy(
            src_ref=end_ref,
            dst_ref=ends.at[sp],
            send_sem=end_send.at[other],
            recv_sem=end_recv.at[sp],
            device_id=(other, tp),
            device_id_type=MESH,
        )

    def end_from(other):
        return pltpu.make_async_remote_copy(
            src_ref=end_ref,
            dst_ref=ends.at[other],
            send_sem=end_send.at[other],
            recv_sem=end_recv.at[other],
            device_id=(other, tp),
            device_id_type=MESH,
        )

    def route_to(other):
        return pltpu.make_async_remote_copy(
            src_ref=routes_ref,
            dst_ref=all_routes.at[sp],
            send_sem=route_send.at[other],
            recv_sem=route_recv.at[sp],
            device_id=(other, tp),
            device_id_type=MESH,
        )

    def route_from(other):
        return pltpu.make_async_remote_copy(
            src_ref=routes_ref,
            dst_ref=all_routes.at[other],
            send_sem=route_send.at[other],
            recv_sem=route_recv.at[other],
            device_id=(other, tp),
            device_id_type=MESH,
        )

    def token_to(other):
        return pltpu.make_async_remote_copy(
            src_ref=mixed_ref.at[other],
            dst_ref=tokens.at[tp],
            send_sem=token_send.at[other],
            recv_sem=token_recv.at[tp],
            device_id=(sp, other),
            device_id_type=MESH,
        )

    def token_from(other):
        return pltpu.make_async_remote_copy(
            src_ref=mixed_ref.at[other],
            dst_ref=tokens.at[other],
            send_sem=token_send.at[other],
            recv_sem=token_recv.at[other],
            device_id=(sp, other),
            device_id_type=MESH,
        )

    def each_sp(action):
        def body(step, carry):
            action(lax.rem(sp + step, sp_count))
            return carry

        lax.fori_loop(1, sp_count, body, 0)

    def each_tp(action):
        def body(step, carry):
            action(lax.rem(tp + step, tp_count))
            return carry

        lax.fori_loop(1, tp_count, body, 0)

    for load in loads[:12]:
        load.wait()
    routes_ref[:top_count] = ids_ref[...].astype(jnp.float32)
    routes_ref[top_count:] = gates_ref[...]
    eye = lax.broadcasted_iota(jnp.int32, (groups, groups), 0) == lax.broadcasted_iota(
        jnp.int32, (groups, groups), 1
    )
    step_size = jnp.exp(jnp.sum(jnp.where(eye, step_ref[...], 0.0), axis=1, keepdims=True))
    decay_real = real_ref[...]
    decay_imag = imag_ref[...]
    magnitude = jnp.exp(decay_real * step_size)
    bar = (magnitude * jnp.cos(decay_imag * step_size), magnitude * jnp.sin(decay_imag * step_size))
    denominator = decay_real * decay_real + decay_imag * decay_imag
    less_one = bar[0] - 1.0
    coef = (
        ((less_one * decay_real + bar[1] * decay_imag) / denominator)[:, None, :],
        ((bar[1] * decay_real - less_one * decay_imag) / denominator)[:, None, :],
    )
    drive = times(coef, (in_re_ref[...], in_im_ref[...]))
    bar = tuple(flatten_rows(part, 8) for part in bar)
    spread = jnp.where(
        jnp.bitwise_and(lax.broadcasted_iota(jnp.int32, (states, wide), 1), states - 1)
        == lax.broadcasted_iota(jnp.int32, (states, wide), 0),
        1.0,
        0.0,
    ).astype(jnp.bfloat16)
    lane = lax.broadcasted_iota(jnp.int32, (channels, wide), 1)
    own = [
        jnp.logical_and(lane >= group * states, lane < (group + 1) * states) for group in range(groups)
    ]

    def scatter(table, target, part):
        for index, piece in enumerate(split_in_two(table.reshape(channel_count, states))):
            tiled = jnp.dot(piece, spread, preferred_element_type=jnp.float32)
            for group in range(groups):
                at = slice(group * channels, (group + 1) * channels)
                target[index, at, part * wide : (part + 1) * wide] = jnp.where(
                    own[group], tiled[at], 0.0
                ).astype(jnp.bfloat16)

    for part in range(2):
        scatter(drive[part], feeds, part)
    scatter(out_re_ref[...], reads, 0)
    scatter(-out_im_ref[...], reads, 1)

    order = lax.broadcasted_iota(jnp.int32, (length, length), 0)
    shuffle = jnp.where(
        lax.broadcasted_iota(jnp.int32, (length, length), 1)
        == jnp.bitwise_and(order, 7) * segment + lax.shift_right_logical(order, 3),
        1.0,
        0.0,
    ).astype(jnp.bfloat16)
    permuted[...] = jnp.dot(shuffle, inputs_ref[...], preferred_element_type=jnp.float32).astype(jnp.bfloat16)
    block = min(512, wide)
    for first in range(0, 2 * wide, block):
        states_ref[:, first : first + block] = jnp.dot(
            permuted[...], feeds[0, :, first : first + block], preferred_element_type=jnp.float32
        ) + jnp.dot(
            permuted[...], feeds[1, :, first : first + block], preferred_element_type=jnp.float32
        )

    def advance(start, keep):
        def body(index, state):
            at = pl.ds(pl.multiple_of(index * 8, 8), 8)
            moved = times(bar, state)
            state = (moved[0] + states_ref[at, :wide], moved[1] + states_ref[at, wide:])
            if keep:
                states_ref[at, :wide] = state[0]
                states_ref[at, wide:] = state[1]
            return state

        return lax.fori_loop(0, segment, body, start, unroll=4)

    zero = jnp.zeros((8, wide), jnp.float32)
    tails = advance((zero, zero), False)
    row = tuple(part[:1] for part in bar)
    power = 1
    while power < segment:
        row = times(row, row)
        power *= 2
    over_segment = row
    while power < length:
        row = times(row, row)
        power *= 2
    over_block = row
    nothing = (zero[:1], zero[:1])
    gathered = nothing
    for index in range(8):
        moved = times(over_segment, gathered)
        gathered = tuple(moved[part] + tails[part][index : index + 1] for part in range(2))
    end_ref[0:1] = gathered[0]
    end_ref[1:2] = gathered[1]
    pl.semaphore_wait(barrier, sp_count - 1 + members - 1)
    each_sp(lambda other: end_to(other).start())
    each_sp(lambda other: route_to(other).start())
    all_routes[sp] = routes_ref[...]
    each_sp(lambda other: end_from(other).wait_recv())
    carried = nothing
    for source in range(sp_count):
        moved = times(over_block, carried)
        earlier = sp > source
        carried = tuple(
            jnp.where(earlier, moved[part] + ends[source, part : part + 1], carried[part]) for part in range(2)
        )
    begins = ([], [])
    for index in range(8):
        for part in range(2):
            begins[part].append(carried[part])
        moved = times(over_segment, carried)
        carried = tuple(moved[part] + tails[part][index : index + 1] for part in range(2))
    advance(tuple(jnp.concatenate(part, axis=0) for part in begins), True)

    gains = flatten_rows(skip_ref[...], 1)
    across = (((1,), (1,)), ((), ()))
    mixed = []
    for first in range(0, length, rows):
        coarse, fine = split_in_two(states_ref[first : first + rows])
        readout = (
            lax.dot_general(coarse, reads[0], across, preferred_element_type=jnp.float32)
            + lax.dot_general(fine, reads[0], across, preferred_element_type=jnp.float32)
            + lax.dot_general(coarse, reads[1], across, preferred_element_type=jnp.float32)
        )
        direct = gains * permuted[first : first + rows].astype(jnp.float32)
        mixed.append(jax.nn.gelu(readout + direct).astype(jnp.bfloat16))
    mixed = jnp.concatenate(mixed, axis=0)
    ordered = lax.dot_general(
        shuffle, mixed, (((0,), (0,)), ((), ())), preferred_element_type=jnp.float32
    ).astype(jnp.bfloat16)
    for other in range(tp_count):
        mixed_ref[other] = ordered[other * rows : (other + 1) * rows]
    each_tp(lambda other: token_to(other).start())
    tokens[tp] = mixed_ref[tp]
    visits = visiting_order(planes)

    def visited(step):
        block = jnp.int32(visits[0][step])
        for own in range(1, planes):
            block = jnp.where(plane == own, visits[own][step], block)
        return block

    steps = [plane] + [visited(step) for step in range(1, planes)]

    def pass_up(block, part):
        return pltpu.make_async_remote_copy(
            src_ref=blocks.at[block * SPLIT + part],
            dst_ref=blocks.at[block * SPLIT + part],
            send_sem=up_sem.at[block * SPLIT + part],
            recv_sem=block_sem.at[block * SPLIT + part],
            device_id=plane_id(jnp.minimum(plane + 1, planes - 1)),
            device_id_type=MESH,
        )

    def pass_down(block, part):
        return pltpu.make_async_remote_copy(
            src_ref=blocks.at[block * SPLIT + part],
            dst_ref=blocks.at[block * SPLIT + part],
            send_sem=down_sem.at[block * SPLIT + part],
            recv_sem=block_sem.at[block * SPLIT + part],
            device_id=plane_id(jnp.maximum(plane - 1, 0)),
            device_id_type=MESH,
        )

    def goes_up(block):
        return jnp.logical_and(block <= plane, plane < planes - 1)

    def goes_down(block):
        return jnp.logical_and(block >= plane, plane > 0)

    def forward(block, part):
        @pl.when(goes_up(block))
        def _():
            pass_up(block, part).start()

        @pl.when(goes_down(block))
        def _():
            pass_down(block, part).start()

    def deal(block, other):
        return pltpu.make_async_remote_copy(
            src_ref=sent.at[block, other],
            dst_ref=arrived.at[block, me],
            send_sem=sent_sem.at[block, other],
            recv_sem=arrived_sem.at[block, me],
            device_id=member_id(other),
            device_id_type=MESH,
        )

    def reply(block, other):
        return pltpu.make_async_remote_copy(
            src_ref=replies.at[block, other],
            dst_ref=returned.at[block, me],
            send_sem=replies_sem.at[block, other],
            recv_sem=returned_sem.at[block, me],
            device_id=member_id(other),
            device_id_type=MESH,
        )

    def landing(buffer, sem, block, other):
        return pltpu.make_async_remote_copy(
            src_ref=buffer.at[block, other],
            dst_ref=buffer.at[block, other],
            send_sem=sem.at[block, other],
            recv_sem=sem.at[block, other],
            device_id=member_id(other),
            device_id_type=MESH,
        )

    def homeward(block, part):
        return pltpu.make_async_remote_copy(
            src_ref=partial.at[block * SHARE + part],
            dst_ref=homed.at[plane * SHARE + part],
            send_sem=partial_sem.at[block * SHARE + part],
            recv_sem=homed_sem.at[plane * SHARE + part],
            device_id=plane_id(block),
            device_id_type=MESH,
        )

    def each_other(action):
        def body(step, carry):
            action(lax.rem(me + step, members))
            return carry

        lax.fori_loop(1, members, body, 0)

    def place(block):
        routes = all_routes[block * rows_y + row_y]
        experts = (lax.broadcasted_iota(jnp.int32, (members, row_count), 0) + plane * members).astype(
            jnp.float32
        )
        named = jnp.zeros((members, row_count), jnp.float32)
        gates = jnp.zeros((members, row_count), jnp.float32)
        for index in range(top_count):
            hit = experts == routes[index : index + 1, :]
            named = named + jnp.where(hit, 1.0, 0.0)
            gates = gates + jnp.where(hit, routes[top_count + index : top_count + index + 1, :], 0.0)
        before = (
            lax.broadcasted_iota(jnp.int32, (row_count, row_count), 0)
            < lax.broadcasted_iota(jnp.int32, (row_count, row_count), 1)
        )
        ranks = jnp.dot(
            named.astype(jnp.bfloat16),
            jnp.where(before, 1.0, 0.0).astype(jnp.bfloat16),
            preferred_element_type=jnp.float32,
        )
        ranks = jnp.where(named > 0.5, ranks, -1.0)
        numbers = lax.broadcasted_iota(jnp.int32, (capacity, row_count), 0).astype(jnp.float32)
        hits = [ranks[other : other + 1, :] == numbers for other in range(members)]
        picked = jnp.concatenate([jnp.where(hit, 1.0, 0.0) for hit in hits], axis=0)
        scaled = jnp.concatenate(
            [jnp.where(hits[other], gates[other : other + 1, :], 0.0) for other in range(members)], axis=0
        )
        coarse = scaled.astype(jnp.bfloat16)
        mix_weights[block, :, :row_count] = coarse
        mix_weights[block, :, row_count:] = (scaled - coarse.astype(jnp.float32)).astype(jnp.bfloat16)
        picks[block] = picked.astype(jnp.bfloat16)

    def relay(step, part):
        pass_up(steps[step], part).wait_recv()
        forward(steps[step], part)

    def dispatch(step, part):
        block = steps[step]
        slab = block * SPLIT + part
        picked = picks[block]
        for first in range(0, part_width, column):
            rows = jnp.dot(
                picked, blocks[slab, :, first : first + column], preferred_element_type=jnp.float32
            )
            for other in range(members):
                sent[slab, other, :, first : first + column] = rows[
                    other * capacity : (other + 1) * capacity
                ].astype(jnp.bfloat16)
        each_other(lambda other: deal(slab, other).start())
        arrived[slab, me] = sent[slab, me]

    def apply_expert(step, part):
        block = steps[step]
        for piece in range(SPLIT):
            slab = block * SPLIT + piece
            each_other(lambda other: landing(arrived, arrived_sem, slab, other).wait_recv())
            for other in range(members):
                wide_rows[
                    other * capacity : (other + 1) * capacity, piece * part_width : (piece + 1) * part_width
                ] = arrived[slab, other].astype(jnp.float32)
        rows = wide_rows[...].astype(jnp.bfloat16)
        gate = jnp.dot(rows, gate_w[0], preferred_element_type=jnp.float32)
        up = jnp.dot(rows, up_w[0], preferred_element_type=jnp.float32)
        hidden = (jax.nn.silu(gate) * up).astype(jnp.bfloat16)
        for piece in range(SHARE):
            slab = block * SHARE + piece
            for first in range(0, share_width, column):
                at = piece * share_width + first
                rows = jnp.dot(hidden, down_w[0, :, at : at + column], preferred_element_type=jnp.float32)
                for other in range(members):
                    replies[slab, other, :, first : first + column] = rows[
                        other * capacity : (other + 1) * capacity
                    ].astype(jnp.bfloat16)
            each_other(lambda other: reply(slab, other).start())
            returned[slab, me] = replies[slab, me]

    def combine(step, part):
        block = steps[step]
        slab = block * SHARE + part
        each_other(lambda other: landing(returned, returned_sem, slab, other).wait_recv())
        weights = mix_weights[block]
        for first in range(0, share_width, column):
            rows = jnp.concatenate(
                [returned[slab, other, :, first : first + column].astype(jnp.float32) for other in range(members)],
                axis=0,
            ).astype(jnp.bfloat16)
            both = lax.dot_general(
                weights, rows, (((0,), (0,)), ((), ())), preferred_element_type=jnp.float32
            )
            added = both[:row_count] + both[row_count:]
            if step == 0:
                at = part * share_width + first
                total[:, at : at + column] += added
            else:
                partial[slab, :, first : first + column] = added.astype(jnp.bfloat16)
        if step > 0:
            homeward(block, part).start()

    def shared(step, part):
        rows = hidden_ref[...]
        gate = jnp.dot(rows, sgate_w[...], preferred_element_type=jnp.float32)
        up = jnp.dot(rows, sup_w[...], preferred_element_type=jnp.float32)
        hidden = (jax.nn.silu(gate) * up).astype(jnp.bfloat16)
        for first in range(0, width, column):
            total[:, first : first + column] += jnp.dot(
                hidden, sdown_w[:, first : first + column], preferred_element_type=jnp.float32
            )

    each_sp(lambda other: route_from(other).wait_recv())
    for block in range(planes):
        place(block)
    for load in loads[12:17]:
        load.wait()
    each_tp(lambda other: token_from(other).wait_recv())
    token_rows = jnp.concatenate([tokens[other] for other in range(tp_count)], axis=1)
    pre_gate = jnp.dot(token_rows, glu_w[...], preferred_element_type=jnp.float32) + bias_ref[...]
    gated = token_rows.astype(jnp.float32) * jax.nn.sigmoid(pre_gate)
    normed = rms_scale(gated, mix_gain_ref[...]).astype(jnp.bfloat16)
    stream = residual_ref[...].astype(jnp.float32) + jnp.dot(
        normed, proj_w[...], preferred_element_type=jnp.float32
    )
    total[...] = stream
    hidden = rms_scale(stream, norm_gain_ref[...]).astype(jnp.bfloat16)
    hidden_ref[...] = hidden
    for part in range(SPLIT):
        blocks[plane * SPLIT + part] = hidden[:, part * part_width : (part + 1) * part_width]
        forward(plane, part)
    for load in loads[17:]:
        load.wait()
    actions = {"A": dispatch, "F": relay, "S": shared, "B": apply_expert, "C": combine}
    for stage, step, part in stages_of(planes):
        actions[stage](step, part)
    for part in range(SHARE):
        at = slice(part * share_width, (part + 1) * share_width)
        result = total[:, at]
        for step in range(1, planes):
            block = steps[step]
            pltpu.make_async_remote_copy(
                src_ref=partial.at[block * SHARE + part],
                dst_ref=homed.at[block * SHARE + part],
                send_sem=partial_sem.at[block * SHARE + part],
                recv_sem=homed_sem.at[block * SHARE + part],
                device_id=plane_id(block),
                device_id_type=MESH,
            ).wait_recv()
            result = result + homed[block * SHARE + part].astype(jnp.float32)
        out_ref[:, at] = result.astype(out_ref.dtype)

    for step in range(planes):
        block = steps[step]
        for part in range(SPLIT):

            @pl.when(goes_up(block))
            def _():
                pass_up(block, part).wait_send()

            @pl.when(goes_down(block))
            def _():
                pass_down(block, part).wait_send()

            each_other(lambda other: deal(block * SPLIT + part, other).wait_send())
        for part in range(SHARE):
            each_other(lambda other: reply(block * SHARE + part, other).wait_send())
            if step > 0:
                homeward(block, part).wait_send()
    each_sp(lambda other: end_to(other).wait_send())
    each_sp(lambda other: route_to(other).wait_send())
    each_tp(lambda other: token_to(other).wait_send())


def layer(arguments, capacity, collective_id):
    sp_count, tp_count = lax.axis_size("sp"), lax.axis_size("tp")
    inputs, residual, input_re = arguments[0], arguments[1], arguments[5]
    length, channel_count = inputs.shape
    groups, channels, states = input_re.shape
    rows, width = residual.shape
    top_count = arguments[10].shape[0]
    wide = groups * states
    planes = planes_of(sp_count)
    members = sp_count * tp_count // planes
    capacity = -(-capacity // 8) * 8
    slots = members * capacity
    hbm = pl.BlockSpec(memory_space=pl.ANY)
    bf16, f32 = jnp.bfloat16, jnp.float32
    vmem, dma = pltpu.VMEM, pltpu.SemaphoreType.DMA
    pieces = vmem((planes * SPLIT, members, capacity, width // SPLIT), bf16)
    shares = vmem((planes * SHARE, members, capacity, width // SHARE), bf16)
    whole = vmem((planes * SPLIT, rows, width // SPLIT), bf16)
    parts = vmem((planes * SHARE, rows, width // SHARE), bf16)
    tables = vmem((2, channel_count, 2 * wide), bf16)
    tokens = vmem((tp_count, rows, channel_count), bf16)
    routes = (2 * top_count, rows)
    return pl.pallas_call(
        functools.partial(layer_kernel, sp_count, tp_count, capacity),
        out_shape=jax.ShapeDtypeStruct((rows, width), bf16),
        in_specs=[hbm] * len(arguments),
        out_specs=pl.BlockSpec(memory_space=pltpu.VMEM),
        scratch_shapes=[vmem(argument.shape, argument.dtype) for argument in arguments]
        + [
            tables,
            tables,
            vmem((length, 2 * wide), f32),
            vmem((length, channel_count), bf16),
            tokens,
            vmem((2, wide), f32),
            vmem((sp_count, 2, wide), f32),
            tokens,
            vmem(routes, f32),
            vmem((sp_count,) + routes, f32),
            vmem((planes, slots, rows), bf16),
            vmem((rows, width), bf16),
            whole,
            pieces,
            pieces,
            shares,
            shares,
            parts,
            parts,
            vmem((planes, slots, 2 * rows), bf16),
            vmem((slots, width), f32),
            vmem((rows, width), f32),
            dma((len(arguments),)),
        ]
        + [dma((sp_count,))] * 4
        + [dma((tp_count,))] * 2
        + [dma((planes * SPLIT,))] * 3
        + [dma((planes * SPLIT, members))] * 2
        + [dma((planes * SHARE, members))] * 2
        + [dma((planes * SHARE,))] * 2,
        compiler_params=pltpu.CompilerParams(
            collective_id=collective_id, has_side_effects=True, vmem_limit_bytes=63 * 2**20
        ),
    )(*arguments)


def on_device(
    mixer_input,
    residual,
    decay_real,
    decay_imag,
    log_step,
    input_re,
    input_im,
    output_re,
    output_im,
    skip_gain,
    glu_weight,
    glu_bias,
    mix_gain,
    out_weight,
    norm_gain,
    route_ids,
    route_gates,
    expert_gate,
    expert_up,
    expert_down,
    shared_gate,
    shared_up,
    shared_down,
):
    row_count, top_count = route_ids.shape
    expert_count = lax.axis_size(("sp", "tp"))
    capacity = max(2, 3 * row_count * top_count // (2 * expert_count))
    arguments = (
        mixer_input,
        residual,
        decay_real,
        decay_imag,
        log_step[None, :],
        jnp.swapaxes(input_re, 1, 2),
        jnp.swapaxes(input_im, 1, 2),
        output_re,
        output_im,
        skip_gain,
        route_ids.T,
        route_gates.T,
        glu_weight,
        glu_bias[None, :],
        mix_gain[None, :],
        out_weight,
        norm_gain[None, :],
        shared_gate,
        shared_up,
        shared_down,
        expert_gate,
        expert_up,
        expert_down,
    )
    return layer(arguments, capacity, 1)


def solution(mesh):
    return jax.shard_map(
        on_device,
        mesh=mesh,
        in_specs=(
            P("sp", "tp"),
            P(("sp", "tp"), None),
            P("tp", None),
            P("tp", None),
            P("tp"),
            P("tp", None, None),
            P("tp", None, None),
            P("tp", None, None),
            P("tp", None, None),
            P("tp", None),
            P(),
            P(),
            P(),
            P(),
            P(),
            P(("sp", "tp"), None),
            P(("sp", "tp"), None),
            P(("sp", "tp"), None, None),
            P(("sp", "tp"), None, None),
            P(("sp", "tp"), None, None),
            P(),
            P(),
            P(),
        ),
        out_specs=P(("sp", "tp"), None),
        check_vma=False,
    )
```

```python
import functools
import math

import jax
import jax.numpy as jnp
from jax import lax
from jax.experimental import pallas as pl
from jax.experimental.pallas import tpu as pltpu
from jax.sharding import PartitionSpec as P

NORM_EPS = 1e-06
HIGHEST = lax.Precision.HIGHEST
MESH = pl.DeviceIdType.MESH


def times(a, b):
    return (a[0] * b[0] - a[1] * b[1], a[0] * b[1] + a[1] * b[0])


def rms_scale(values, gain):
    return values * lax.rsqrt(jnp.mean(values * values, axis=-1, keepdims=True) + NORM_EPS) * gain


def flatten_rows(values, count):
    groups, states = values.shape
    width = groups * states
    lanes = lax.broadcasted_iota(jnp.int32, (states, width), 1)
    spread = jnp.where(
        jnp.bitwise_and(lanes, states - 1) == lax.broadcasted_iota(jnp.int32, (states, width), 0), 1.0, 0.0
    )
    tiled = jnp.dot(values, spread, precision=HIGHEST, preferred_element_type=jnp.float32)
    first = lax.broadcasted_iota(jnp.int32, (groups, width), 0) * states
    lanes = lax.broadcasted_iota(jnp.int32, (groups, width), 1)
    own = jnp.logical_and(lanes >= first, lanes < first + states)
    row = jnp.sum(jnp.where(own, tiled, 0.0), axis=0, keepdims=True)
    return jnp.broadcast_to(row, (count, width))


def split_in_two(values):
    coarse = values.astype(jnp.bfloat16)
    return coarse, (values - coarse.astype(jnp.float32)).astype(jnp.bfloat16)


SPLIT = 2
SHARE = 2
STAGES = (
    "A00S00A01F10A10F20A20F11A11F21A21F30A30F31",
    "A31B20B30C20B10C21C30B00C31M20C10M21C11M30",
    "C00C01M31",
)


def stages_of(planes):
    if planes == 4:
        return [
            (text[at], int(text[at + 1]), int(text[at + 2])) for text in STAGES for at in range(0, len(text), 3)
        ]
    stages = [("A", 0, part) for part in range(SPLIT)] + [("S", 0, 0)]
    for step in range(1, planes):
        stages += [(stage, step, part) for part in range(SPLIT) for stage in "FA"]
        stages += [("B", step, 0)] + [("C", step, part) for part in range(SHARE)]
    return stages + [("B", 0, 0)] + [("C", 0, part) for part in range(SHARE)]


def planes_of(sp_count):
    return math.gcd(sp_count, 4)


def visiting_order(planes):
    if planes == 4:
        return [[0, 1, 2, 3], [1, 0, 2, 3], [2, 3, 1, 0], [3, 2, 1, 0]]
    return [sorted(range(planes), key=lambda other: (abs(other - own), -other)) for own in range(planes)]


def layer_kernel(
    sp_count,
    tp_count,
    capacity,
    *refs,
):
    sources = refs[:23]
    out_ref = refs[23]
    held = refs[24:47]
    (
        inputs_ref,
        residual_ref,
        real_ref,
        imag_ref,
        step_ref,
        in_re_ref,
        in_im_ref,
        out_re_ref,
        out_im_ref,
        skip_ref,
        ids_ref,
        gates_ref,
        glu_w,
        bias_ref,
        mix_gain_ref,
        proj_w,
        norm_gain_ref,
        sgate_w,
        sup_w,
        sdown_w,
        gate_w,
        up_w,
        down_w,
    ) = held
    (
        feeds,
        reads,
        states_ref,
        permuted,
        mixed_ref,
        end_ref,
        ends,
        tokens,
        routes_ref,
        all_routes,
        picks,
        hidden_ref,
        blocks,
        sent,
        arrived,
        replies,
        returned,
        partial,
        homed,
        mix_weights,
        kept,
        joined,
        wide_rows,
        total,
        load_sem,
        end_send,
        end_recv,
        route_send,
        route_recv,
        token_send,
        token_recv,
        up_sem,
        down_sem,
        block_sem,
        sent_sem,
        arrived_sem,
        replies_sem,
        returned_sem,
        partial_sem,
        homed_sem,
        joined_sem,
    ) = refs[47:]
    sp = lax.axis_index("sp")
    tp = lax.axis_index("tp")
    length, channel_count = inputs_ref.shape
    groups, channels, states = in_re_ref.shape
    wide = groups * states
    segment = length // 8
    rows = length // tp_count
    planes = planes_of(sp_count)
    rows_y = sp_count // planes
    members = rows_y * tp_count
    width = residual_ref.shape[1]
    row_count = rows
    top_count = ids_ref.shape[0]
    part_width = width // SPLIT
    share_width = width // SHARE
    column = min(512, part_width, share_width)
    plane = sp // rows_y
    row_y = lax.rem(sp, rows_y)
    me = row_y * tp_count + tp

    barrier = pltpu.get_barrier_semaphore()

    def greet_sp(step, carry):
        pl.semaphore_signal(
            barrier, inc=1, device_id=(lax.rem(sp + step, sp_count), tp), device_id_type=MESH
        )
        return carry

    def member_id(other):
        return (plane * rows_y + other // tp_count, lax.rem(other, tp_count))

    def plane_id(other):
        return (other * rows_y + row_y, tp)

    def greet_member(step, carry):
        pl.semaphore_signal(
            barrier, inc=1, device_id=member_id(lax.rem(me + step, members)), device_id_type=MESH
        )
        return carry

    loads = [
        pltpu.make_async_copy(source, target, load_sem.at[number])
        for number, (source, target) in enumerate(zip(sources, held))
    ]
    for load in loads:
        load.start()
    lax.fori_loop(1, sp_count, greet_sp, 0)
    lax.fori_loop(1, members, greet_member, 0)
    def end_to(other):
        return pltpu.make_async_remote_copy(
            src_ref=end_ref,
            dst_ref=ends.at[sp],
            send_sem=end_send.at[other],
            recv_sem=end_recv.at[sp],
            device_id=(other, tp),
            device_id_type=MESH,
        )

    def end_from(other):
        return pltpu.make_async_remote_copy(
            src_ref=end_ref,
            dst_ref=ends.at[other],
            send_sem=end_send.at[other],
            recv_sem=end_recv.at[other],
            device_id=(other, tp),
            device_id_type=MESH,
        )

    def route_to(other):
        return pltpu.make_async_remote_copy(
            src_ref=routes_ref,
            dst_ref=all_routes.at[sp],
            send_sem=route_send.at[other],
            recv_sem=route_recv.at[sp],
            device_id=(other, tp),
            device_id_type=MESH,
        )

    def route_from(other):
        return pltpu.make_async_remote_copy(
            src_ref=routes_ref,
            dst_ref=all_routes.at[other],
            send_sem=route_send.at[other],
            recv_sem=route_recv.at[other],
            device_id=(other, tp),
            device_id_type=MESH,
        )

    def token_to(other):
        return pltpu.make_async_remote_copy(
            src_ref=mixed_ref.at[other],
            dst_ref=tokens.at[tp],
            send_sem=token_send.at[other],
            recv_sem=token_recv.at[tp],
            device_id=(sp, other),
            device_id_type=MESH,
        )

    def token_from(other):
        return pltpu.make_async_remote_copy(
            src_ref=mixed_ref.at[other],
            dst_ref=tokens.at[other],
            send_sem=token_send.at[other],
            recv_sem=token_recv.at[other],
            device_id=(sp, other),
            device_id_type=MESH,
        )

    def each_sp(action):
        def body(step, carry):
            action(lax.rem(sp + step, sp_count))
            return carry

        lax.fori_loop(1, sp_count, body, 0)

    def each_tp(action):
        def body(step, carry):
            action(lax.rem(tp + step, tp_count))
            return carry

        lax.fori_loop(1, tp_count, body, 0)

    for load in loads[:12]:
        load.wait()
    routes_ref[:top_count] = ids_ref[...].astype(jnp.float32)
    routes_ref[top_count:] = gates_ref[...]
    eye = lax.broadcasted_iota(jnp.int32, (groups, groups), 0) == lax.broadcasted_iota(
        jnp.int32, (groups, groups), 1
    )
    step_size = jnp.exp(jnp.sum(jnp.where(eye, step_ref[...], 0.0), axis=1, keepdims=True))
    decay_real = real_ref[...]
    decay_imag = imag_ref[...]
    magnitude = jnp.exp(decay_real * step_size)
    bar = (magnitude * jnp.cos(decay_imag * step_size), magnitude * jnp.sin(decay_imag * step_size))
    denominator = decay_real * decay_real + decay_imag * decay_imag
    less_one = bar[0] - 1.0
    coef = (
        ((less_one * decay_real + bar[1] * decay_imag) / denominator)[:, None, :],
        ((bar[1] * decay_real - less_one * decay_imag) / denominator)[:, None, :],
    )
    drive = times(coef, (in_re_ref[...], in_im_ref[...]))
    bar = tuple(flatten_rows(part, 8) for part in bar)
    spread = jnp.where(
        jnp.bitwise_and(lax.broadcasted_iota(jnp.int32, (states, wide), 1), states - 1)
        == lax.broadcasted_iota(jnp.int32, (states, wide), 0),
        1.0,
        0.0,
    ).astype(jnp.bfloat16)
    lane = lax.broadcasted_iota(jnp.int32, (channels, wide), 1)
    own = [
        jnp.logical_and(lane >= group * states, lane < (group + 1) * states) for group in range(groups)
    ]

    def scatter(table, target, part):
        for index, piece in enumerate(split_in_two(table.reshape(channel_count, states))):
            tiled = jnp.dot(piece, spread, preferred_element_type=jnp.float32)
            for group in range(groups):
                at = slice(group * channels, (group + 1) * channels)
                target[index, at, part * wide : (part + 1) * wide] = jnp.where(
                    own[group], tiled[at], 0.0
                ).astype(jnp.bfloat16)

    for part in range(2):
        scatter(drive[part], feeds, part)
    turn = jnp.where(
        lax.broadcasted_iota(jnp.int32, (states, states), 0)
        == lax.broadcasted_iota(jnp.int32, (states, states), 1),
        1.0,
        0.0,
    ).astype(jnp.bfloat16)
    across = (((1,), (1,)), ((), ()))
    channel = lax.broadcasted_iota(jnp.int32, (states, channel_count), 1)
    for part, table in enumerate((out_re_ref[...], -out_im_ref[...])):
        for index, piece in enumerate(split_in_two(table.reshape(channel_count, states))):
            turned = lax.dot_general(turn, piece, across, preferred_element_type=jnp.float32)
            for group in range(groups):
                here = jnp.logical_and(channel >= group * channels, channel < (group + 1) * channels)
                at = part * wide + group * states
                reads[index, at : at + states] = jnp.where(here, turned, 0.0).astype(jnp.bfloat16)

    order = lax.broadcasted_iota(jnp.int32, (length, length), 0)
    shuffle = jnp.where(
        lax.broadcasted_iota(jnp.int32, (length, length), 1)
        == jnp.bitwise_and(order, 7) * segment + lax.shift_right_logical(order, 3),
        1.0,
        0.0,
    ).astype(jnp.bfloat16)
    permuted[...] = jnp.dot(shuffle, inputs_ref[...], preferred_element_type=jnp.float32).astype(jnp.bfloat16)
    block = min(512, wide)
    for first in range(0, 2 * wide, block):
        states_ref[:, first : first + block] = jnp.dot(
            permuted[...], feeds[0, :, first : first + block], preferred_element_type=jnp.float32
        ) + jnp.dot(
            permuted[...], feeds[1, :, first : first + block], preferred_element_type=jnp.float32
        )

    def advance(start, keep):
        def body(index, state):
            at = pl.ds(pl.multiple_of(index * 8, 8), 8)
            moved = times(bar, state)
            state = (moved[0] + states_ref[at, :wide], moved[1] + states_ref[at, wide:])
            if keep:
                states_ref[at, :wide] = state[0]
                states_ref[at, wide:] = state[1]
            return state

        return lax.fori_loop(0, segment, body, start, unroll=4)

    zero = jnp.zeros((8, wide), jnp.float32)
    tails = advance((zero, zero), False)
    row = tuple(part[:1] for part in bar)
    power = 1
    while power < segment:
        row = times(row, row)
        power *= 2
    over_segment = row
    while power < length:
        row = times(row, row)
        power *= 2
    over_block = row
    nothing = (zero[:1], zero[:1])
    gathered = nothing
    for index in range(8):
        moved = times(over_segment, gathered)
        gathered = tuple(moved[part] + tails[part][index : index + 1] for part in range(2))
    end_ref[0:1] = gathered[0]
    end_ref[1:2] = gathered[1]
    pl.semaphore_wait(barrier, sp_count - 1 + members - 1)
    each_sp(lambda other: end_to(other).start())
    each_sp(lambda other: route_to(other).start())
    all_routes[sp] = routes_ref[...]
    each_sp(lambda other: end_from(other).wait_recv())
    carried = nothing
    for source in range(sp_count):
        moved = times(over_block, carried)
        earlier = sp > source
        carried = tuple(
            jnp.where(earlier, moved[part] + ends[source, part : part + 1], carried[part]) for part in range(2)
        )
    begins = ([], [])
    for index in range(8):
        for part in range(2):
            begins[part].append(carried[part])
        moved = times(over_segment, carried)
        carried = tuple(moved[part] + tails[part][index : index + 1] for part in range(2))
    advance(tuple(jnp.concatenate(part, axis=0) for part in begins), True)

    gains = flatten_rows(skip_ref[...], 1)
    mixed = []
    for first in range(0, length, rows):
        coarse, fine = split_in_two(states_ref[first : first + rows])
        readout = (
            jnp.dot(coarse, reads[0], preferred_element_type=jnp.float32)
            + jnp.dot(fine, reads[0], preferred_element_type=jnp.float32)
            + jnp.dot(coarse, reads[1], preferred_element_type=jnp.float32)
        )
        direct = gains * permuted[first : first + rows].astype(jnp.float32)
        mixed.append(jax.nn.gelu(readout + direct).astype(jnp.bfloat16))
    mixed = jnp.concatenate(mixed, axis=0)
    ordered = lax.dot_general(
        shuffle, mixed, (((0,), (0,)), ((), ())), preferred_element_type=jnp.float32
    ).astype(jnp.bfloat16)
    for other in range(tp_count):
        mixed_ref[other] = ordered[other * rows : (other + 1) * rows]
    each_tp(lambda other: token_to(other).start())
    tokens[tp] = mixed_ref[tp]
    visits = visiting_order(planes)

    def visited(step):
        block = jnp.int32(visits[0][step])
        for own in range(1, planes):
            block = jnp.where(plane == own, visits[own][step], block)
        return block

    steps = [plane] + [visited(step) for step in range(1, planes)]

    def pass_up(block, part):
        return pltpu.make_async_remote_copy(
            src_ref=blocks.at[block * SPLIT + part],
            dst_ref=blocks.at[block * SPLIT + part],
            send_sem=up_sem.at[block * SPLIT + part],
            recv_sem=block_sem.at[block * SPLIT + part],
            device_id=plane_id(jnp.minimum(plane + 1, planes - 1)),
            device_id_type=MESH,
        )

    def pass_down(block, part):
        return pltpu.make_async_remote_copy(
            src_ref=blocks.at[block * SPLIT + part],
            dst_ref=blocks.at[block * SPLIT + part],
            send_sem=down_sem.at[block * SPLIT + part],
            recv_sem=block_sem.at[block * SPLIT + part],
            device_id=plane_id(jnp.maximum(plane - 1, 0)),
            device_id_type=MESH,
        )

    def goes_up(block):
        return jnp.logical_and(block <= plane, plane < planes - 1)

    def goes_down(block):
        return jnp.logical_and(block >= plane, plane > 0)

    def forward(block, part):
        @pl.when(goes_up(block))
        def _():
            pass_up(block, part).start()

        @pl.when(goes_down(block))
        def _():
            pass_down(block, part).start()

    def deal(block, other):
        return pltpu.make_async_remote_copy(
            src_ref=sent.at[block, other],
            dst_ref=arrived.at[block, me],
            send_sem=sent_sem.at[block, other],
            recv_sem=arrived_sem.at[block, me],
            device_id=member_id(other),
            device_id_type=MESH,
        )

    def reply(block, other):
        return pltpu.make_async_remote_copy(
            src_ref=replies.at[block, other],
            dst_ref=returned.at[block, me],
            send_sem=replies_sem.at[block, other],
            recv_sem=returned_sem.at[block, me],
            device_id=member_id(other),
            device_id_type=MESH,
        )

    def landing(buffer, sem, block, other):
        return pltpu.make_async_remote_copy(
            src_ref=buffer.at[block, other],
            dst_ref=buffer.at[block, other],
            send_sem=sem.at[block, other],
            recv_sem=sem.at[block, other],
            device_id=member_id(other),
            device_id_type=MESH,
        )

    def homeward(block, part):
        return pltpu.make_async_remote_copy(
            src_ref=partial.at[block * SHARE + part],
            dst_ref=homed.at[plane * SHARE + part],
            send_sem=partial_sem.at[block * SHARE + part],
            recv_sem=homed_sem.at[plane * SHARE + part],
            device_id=plane_id(block),
            device_id_type=MESH,
        )

    joins = planes == 4
    inner = jnp.logical_and(plane > 0, plane < planes - 1)
    beside = plane + 1 - 2 * lax.rem(plane, 2)

    def join(block, step, part):
        slot = (step - 2) * SHARE + part
        return pltpu.make_async_remote_copy(
            src_ref=partial.at[block * SHARE + part],
            dst_ref=joined.at[slot],
            send_sem=partial_sem.at[block * SHARE + part],
            recv_sem=joined_sem.at[slot],
            device_id=plane_id(beside),
            device_id_type=MESH,
        )

    def each_other(action):
        def body(step, carry):
            action(lax.rem(me + step, members))
            return carry

        lax.fori_loop(1, members, body, 0)

    def place(block):
        routes = all_routes[block * rows_y + row_y]
        experts = (lax.broadcasted_iota(jnp.int32, (members, row_count), 0) + plane * members).astype(
            jnp.float32
        )
        named = jnp.zeros((members, row_count), jnp.float32)
        gates = jnp.zeros((members, row_count), jnp.float32)
        for index in range(top_count):
            hit = experts == routes[index : index + 1, :]
            named = named + jnp.where(hit, 1.0, 0.0)
            gates = gates + jnp.where(hit, routes[top_count + index : top_count + index + 1, :], 0.0)
        before = (
            lax.broadcasted_iota(jnp.int32, (row_count, row_count), 0)
            < lax.broadcasted_iota(jnp.int32, (row_count, row_count), 1)
        )
        ranks = jnp.dot(
            named.astype(jnp.bfloat16),
            jnp.where(before, 1.0, 0.0).astype(jnp.bfloat16),
            preferred_element_type=jnp.float32,
        )
        ranks = jnp.where(named > 0.5, ranks, -1.0)
        numbers = lax.broadcasted_iota(jnp.int32, (capacity, row_count), 0).astype(jnp.float32)
        hits = [ranks[other : other + 1, :] == numbers for other in range(members)]
        picked = jnp.concatenate([jnp.where(hit, 1.0, 0.0) for hit in hits], axis=0)
        scaled = jnp.concatenate(
            [jnp.where(hits[other], gates[other : other + 1, :], 0.0) for other in range(members)], axis=0
        )
        coarse = scaled.astype(jnp.bfloat16)
        mix_weights[block, :, :row_count] = coarse
        mix_weights[block, :, row_count:] = (scaled - coarse.astype(jnp.float32)).astype(jnp.bfloat16)
        picks[block] = picked.astype(jnp.bfloat16)

    def relay(step, part):
        pass_up(steps[step], part).wait_recv()
        forward(steps[step], part)

    def dispatch(step, part):
        block = steps[step]
        slab = block * SPLIT + part
        picked = picks[block]
        for first in range(0, part_width, column):
            rows = jnp.dot(
                picked, blocks[slab, :, first : first + column], preferred_element_type=jnp.float32
            )
            for other in range(members):
                sent[slab, other, :, first : first + column] = rows[
                    other * capacity : (other + 1) * capacity
                ].astype(jnp.bfloat16)
        each_other(lambda other: deal(slab, other).start())
        arrived[slab, me] = sent[slab, me]

    def apply_expert(step, part):
        block = steps[step]
        for piece in range(SPLIT):
            slab = block * SPLIT + piece
            each_other(lambda other: landing(arrived, arrived_sem, slab, other).wait_recv())
            for other in range(members):
                wide_rows[
                    other * capacity : (other + 1) * capacity, piece * part_width : (piece + 1) * part_width
                ] = arrived[slab, other].astype(jnp.float32)
        rows = wide_rows[...].astype(jnp.bfloat16)
        gate = jnp.dot(rows, gate_w[0], preferred_element_type=jnp.float32)
        up = jnp.dot(rows, up_w[0], preferred_element_type=jnp.float32)
        hidden = (jax.nn.silu(gate) * up).astype(jnp.bfloat16)
        for piece in range(SHARE):
            slab = block * SHARE + piece
            for first in range(0, share_width, column):
                at = piece * share_width + first
                rows = jnp.dot(hidden, down_w[0, :, at : at + column], preferred_element_type=jnp.float32)
                for other in range(members):
                    replies[slab, other, :, first : first + column] = rows[
                        other * capacity : (other + 1) * capacity
                    ].astype(jnp.bfloat16)
            each_other(lambda other: reply(slab, other).start())
            returned[slab, me] = replies[slab, me]

    def combine(step, part):
        block = steps[step]
        slab = block * SHARE + part
        each_other(lambda other: landing(returned, returned_sem, slab, other).wait_recv())
        weights = mix_weights[block]
        for first in range(0, share_width, column):
            rows = jnp.concatenate(
                [returned[slab, other, :, first : first + column].astype(jnp.float32) for other in range(members)],
                axis=0,
            ).astype(jnp.bfloat16)
            both = lax.dot_general(
                weights, rows, (((0,), (0,)), ((), ())), preferred_element_type=jnp.float32
            )
            added = both[:row_count] + both[row_count:]
            if step == 0:
                at = part * share_width + first
                total[:, at : at + column] += added
            else:
                partial[slab, :, first : first + column] = added.astype(jnp.bfloat16)
                if joins and step > 1:
                    kept[(step - 2) * SHARE + part, :, first : first + column] = added
        if joins and step > 1:

            @pl.when(jnp.logical_not(inner))
            def _():
                join(block, step, part).start()

        elif step > 0:
            homeward(block, part).start()

    def merge(step, part):
        block = steps[step]
        slot = (step - 2) * SHARE + part

        @pl.when(inner)
        def _():
            join(block, step, part).wait_recv()
            partial[block * SHARE + part] = (kept[slot] + joined[slot].astype(jnp.float32)).astype(jnp.bfloat16)
            homeward(block, part).start()

    def shared(step, part):
        rows = hidden_ref[...]
        gate = jnp.dot(rows, sgate_w[...], preferred_element_type=jnp.float32)
        up = jnp.dot(rows, sup_w[...], preferred_element_type=jnp.float32)
        hidden = (jax.nn.silu(gate) * up).astype(jnp.bfloat16)
        for first in range(0, width, column):
            total[:, first : first + column] += jnp.dot(
                hidden, sdown_w[:, first : first + column], preferred_element_type=jnp.float32
            )

    each_sp(lambda other: route_from(other).wait_recv())
    for block in range(planes):
        place(block)
    for load in loads[12:17]:
        load.wait()
    each_tp(lambda other: token_from(other).wait_recv())
    token_rows = jnp.concatenate([tokens[other] for other in range(tp_count)], axis=1)
    pre_gate = jnp.dot(token_rows, glu_w[...], preferred_element_type=jnp.float32) + bias_ref[...]
    gated = token_rows.astype(jnp.float32) * jax.nn.sigmoid(pre_gate)
    normed = rms_scale(gated, mix_gain_ref[...]).astype(jnp.bfloat16)
    stream = residual_ref[...].astype(jnp.float32) + jnp.dot(
        normed, proj_w[...], preferred_element_type=jnp.float32
    )
    total[...] = stream
    hidden = rms_scale(stream, norm_gain_ref[...]).astype(jnp.bfloat16)
    hidden_ref[...] = hidden
    for part in range(SPLIT):
        blocks[plane * SPLIT + part] = hidden[:, part * part_width : (part + 1) * part_width]
        forward(plane, part)
    for load in loads[17:]:
        load.wait()
    actions = {"A": dispatch, "F": relay, "S": shared, "B": apply_expert, "C": combine, "M": merge}
    for stage, step, part in stages_of(planes):
        actions[stage](step, part)
    senders = [beside, jnp.where(plane < 2, 2, 1)] if joins else steps[1:]
    for part in range(SHARE):
        at = slice(part * share_width, (part + 1) * share_width)
        result = total[:, at]
        for source in senders:
            pltpu.make_async_remote_copy(
                src_ref=partial.at[source * SHARE + part],
                dst_ref=homed.at[source * SHARE + part],
                send_sem=partial_sem.at[source * SHARE + part],
                recv_sem=homed_sem.at[source * SHARE + part],
                device_id=plane_id(source),
                device_id_type=MESH,
            ).wait_recv()
            result = result + homed[source * SHARE + part].astype(jnp.float32)
        out_ref[:, at] = result.astype(out_ref.dtype)

    for step in range(planes):
        block = steps[step]
        for part in range(SPLIT):

            @pl.when(goes_up(block))
            def _():
                pass_up(block, part).wait_send()

            @pl.when(goes_down(block))
            def _():
                pass_down(block, part).wait_send()

            each_other(lambda other: deal(block * SPLIT + part, other).wait_send())
        for part in range(SHARE):
            each_other(lambda other: reply(block * SHARE + part, other).wait_send())
            if step > 0:
                homeward(block, part).wait_send()
    each_sp(lambda other: end_to(other).wait_send())
    each_sp(lambda other: route_to(other).wait_send())
    each_tp(lambda other: token_to(other).wait_send())


def layer(arguments, capacity, collective_id):
    sp_count, tp_count = lax.axis_size("sp"), lax.axis_size("tp")
    inputs, residual, input_re = arguments[0], arguments[1], arguments[5]
    length, channel_count = inputs.shape
    groups, channels, states = input_re.shape
    rows, width = residual.shape
    top_count = arguments[10].shape[0]
    wide = groups * states
    planes = planes_of(sp_count)
    members = sp_count * tp_count // planes
    capacity = -(-capacity // 8) * 8
    slots = members * capacity
    hbm = pl.BlockSpec(memory_space=pl.ANY)
    bf16, f32 = jnp.bfloat16, jnp.float32
    vmem, dma = pltpu.VMEM, pltpu.SemaphoreType.DMA
    pieces = vmem((planes * SPLIT, members, capacity, width // SPLIT), bf16)
    shares = vmem((planes * SHARE, members, capacity, width // SHARE), bf16)
    whole = vmem((planes * SPLIT, rows, width // SPLIT), bf16)
    parts = vmem((planes * SHARE, rows, width // SHARE), bf16)
    tables = vmem((2, channel_count, 2 * wide), bf16)
    tokens = vmem((tp_count, rows, channel_count), bf16)
    routes = (2 * top_count, rows)
    return pl.pallas_call(
        functools.partial(layer_kernel, sp_count, tp_count, capacity),
        out_shape=jax.ShapeDtypeStruct((rows, width), bf16),
        in_specs=[hbm] * len(arguments),
        out_specs=pl.BlockSpec(memory_space=pltpu.VMEM),
        scratch_shapes=[vmem(argument.shape, argument.dtype) for argument in arguments]
        + [
            tables,
            vmem((2, 2 * wide, channel_count), bf16),
            vmem((length, 2 * wide), f32),
            vmem((length, channel_count), bf16),
            tokens,
            vmem((2, wide), f32),
            vmem((sp_count, 2, wide), f32),
            tokens,
            vmem(routes, f32),
            vmem((sp_count,) + routes, f32),
            vmem((planes, slots, rows), bf16),
            vmem((rows, width), bf16),
            whole,
            pieces,
            pieces,
            shares,
            shares,
            parts,
            parts,
            vmem((planes, slots, 2 * rows), bf16),
            vmem((2 * SHARE, rows, width // SHARE), f32),
            vmem((2 * SHARE, rows, width // SHARE), bf16),
            vmem((slots, width), f32),
            vmem((rows, width), f32),
            dma((len(arguments),)),
        ]
        + [dma((sp_count,))] * 4
        + [dma((tp_count,))] * 2
        + [dma((planes * SPLIT,))] * 3
        + [dma((planes * SPLIT, members))] * 2
        + [dma((planes * SHARE, members))] * 2
        + [dma((planes * SHARE,))] * 2
        + [dma((2 * SHARE,))],
        compiler_params=pltpu.CompilerParams(
            collective_id=collective_id, has_side_effects=True, vmem_limit_bytes=63 * 2**20
        ),
    )(*arguments)


def on_device(
    mixer_input,
    residual,
    decay_real,
    decay_imag,
    log_step,
    input_re,
    input_im,
    output_re,
    output_im,
    skip_gain,
    glu_weight,
    glu_bias,
    mix_gain,
    out_weight,
    norm_gain,
    route_ids,
    route_gates,
    expert_gate,
    expert_up,
    expert_down,
    shared_gate,
    shared_up,
    shared_down,
):
    row_count, top_count = route_ids.shape
    expert_count = lax.axis_size(("sp", "tp"))
    capacity = max(2, 3 * row_count * top_count // (2 * expert_count))
    arguments = (
        mixer_input,
        residual,
        decay_real,
        decay_imag,
        log_step[None, :],
        jnp.swapaxes(input_re, 1, 2),
        jnp.swapaxes(input_im, 1, 2),
        output_re,
        output_im,
        skip_gain,
        route_ids.T,
        route_gates.T,
        glu_weight,
        glu_bias[None, :],
        mix_gain[None, :],
        out_weight,
        norm_gain[None, :],
        shared_gate,
        shared_up,
        shared_down,
        expert_gate,
        expert_up,
        expert_down,
    )
    return layer(arguments, capacity, 1)


def solution(mesh):
    return jax.shard_map(
        on_device,
        mesh=mesh,
        in_specs=(
            P("sp", "tp"),
            P(("sp", "tp"), None),
            P("tp", None),
            P("tp", None),
            P("tp"),
            P("tp", None, None),
            P("tp", None, None),
            P("tp", None, None),
            P("tp", None, None),
            P("tp", None),
            P(),
            P(),
            P(),
            P(),
            P(),
            P(("sp", "tp"), None),
            P(("sp", "tp"), None),
            P(("sp", "tp"), None, None),
            P(("sp", "tp"), None, None),
            P(("sp", "tp"), None, None),
            P(),
            P(),
            P(),
        ),
        out_specs=P(("sp", "tp"), None),
        check_vma=False,
    )
```

```python
import functools
import math

import jax
import jax.numpy as jnp
from jax import lax
from jax.experimental import pallas as pl
from jax.experimental.pallas import tpu as pltpu
from jax.sharding import PartitionSpec as P

NORM_EPS = 1e-06
HIGHEST = lax.Precision.HIGHEST
MESH = pl.DeviceIdType.MESH


def times(a, b):
    return (a[0] * b[0] - a[1] * b[1], a[0] * b[1] + a[1] * b[0])


def rms_scale(values, gain):
    return values * lax.rsqrt(jnp.mean(values * values, axis=-1, keepdims=True) + NORM_EPS) * gain


def flatten_rows(values, count):
    groups, states = values.shape
    width = groups * states
    lanes = lax.broadcasted_iota(jnp.int32, (states, width), 1)
    spread = jnp.where(
        jnp.bitwise_and(lanes, states - 1) == lax.broadcasted_iota(jnp.int32, (states, width), 0), 1.0, 0.0
    )
    tiled = jnp.dot(values, spread, precision=HIGHEST, preferred_element_type=jnp.float32)
    first = lax.broadcasted_iota(jnp.int32, (groups, width), 0) * states
    lanes = lax.broadcasted_iota(jnp.int32, (groups, width), 1)
    own = jnp.logical_and(lanes >= first, lanes < first + states)
    row = jnp.sum(jnp.where(own, tiled, 0.0), axis=0, keepdims=True)
    return jnp.broadcast_to(row, (count, width))


def split_in_two(values):
    coarse = values.astype(jnp.bfloat16)
    return coarse, (values - coarse.astype(jnp.float32)).astype(jnp.bfloat16)


SPLIT = 2
SHARE = 2
STAGES = (
    "A00S00A01F10A10F20A20F11A11F21A21F30A30F31",
    "A31B20B30C20B10C21C30B00C31M20C10M21C11M30",
    "C00C01M31",
)


def stages_of(planes):
    if planes == 4:
        return [
            (text[at], int(text[at + 1]), int(text[at + 2])) for text in STAGES for at in range(0, len(text), 3)
        ]
    stages = [("A", 0, part) for part in range(SPLIT)] + [("S", 0, 0)]
    for step in range(1, planes):
        stages += [(stage, step, part) for part in range(SPLIT) for stage in "FA"]
        stages += [("B", step, 0)] + [("C", step, part) for part in range(SHARE)]
    return stages + [("B", 0, 0)] + [("C", 0, part) for part in range(SHARE)]


def planes_of(sp_count):
    return math.gcd(sp_count, 4)


def visiting_order(planes):
    if planes == 4:
        return [[0, 1, 2, 3], [1, 0, 2, 3], [2, 3, 1, 0], [3, 2, 1, 0]]
    return [sorted(range(planes), key=lambda other: (abs(other - own), -other)) for own in range(planes)]


def layer_kernel(
    sp_count,
    tp_count,
    capacity,
    *refs,
):
    sources = refs[:23]
    out_ref = refs[23]
    held = refs[24:47]
    (
        inputs_ref,
        residual_ref,
        real_ref,
        imag_ref,
        step_ref,
        in_re_ref,
        in_im_ref,
        out_re_ref,
        out_im_ref,
        skip_ref,
        ids_ref,
        gates_ref,
        glu_w,
        bias_ref,
        mix_gain_ref,
        proj_w,
        norm_gain_ref,
        sgate_w,
        sup_w,
        sdown_w,
        gate_w,
        up_w,
        down_w,
    ) = held
    (
        feeds,
        reads,
        states_ref,
        permuted,
        mixed_ref,
        end_ref,
        ends,
        tokens,
        routes_ref,
        all_routes,
        picks,
        hidden_ref,
        blocks,
        sent,
        arrived,
        replies,
        returned,
        partial,
        homed,
        mix_weights,
        kept,
        joined,
        wide_rows,
        total,
        load_sem,
        end_send,
        end_recv,
        route_send,
        route_recv,
        token_send,
        token_recv,
        up_sem,
        down_sem,
        block_sem,
        sent_sem,
        arrived_sem,
        replies_sem,
        returned_sem,
        partial_sem,
        homed_sem,
        joined_sem,
    ) = refs[47:]
    sp = lax.axis_index("sp")
    tp = lax.axis_index("tp")
    length, channel_count = inputs_ref.shape
    groups, channels, states = in_re_ref.shape
    wide = groups * states
    segment = length // 8
    rows = length // tp_count
    planes = planes_of(sp_count)
    rows_y = sp_count // planes
    members = rows_y * tp_count
    width = residual_ref.shape[1]
    row_count = rows
    top_count = ids_ref.shape[0]
    part_width = width // SPLIT
    share_width = width // SHARE
    column = min(512, part_width, share_width)
    plane = sp // rows_y
    row_y = lax.rem(sp, rows_y)
    me = row_y * tp_count + tp

    barrier = pltpu.get_barrier_semaphore()

    def greet_sp(step, carry):
        pl.semaphore_signal(
            barrier, inc=1, device_id=(lax.rem(sp + step, sp_count), tp), device_id_type=MESH
        )
        return carry

    def member_id(other):
        return (plane * rows_y + other // tp_count, lax.rem(other, tp_count))

    def plane_id(other):
        return (other * rows_y + row_y, tp)

    def greet_member(step, carry):
        pl.semaphore_signal(
            barrier, inc=1, device_id=member_id(lax.rem(me + step, members)), device_id_type=MESH
        )
        return carry

    loads = [
        pltpu.make_async_copy(source, target, load_sem.at[number])
        for number, (source, target) in enumerate(zip(sources, held))
    ]
    for load in loads:
        load.start()
    lax.fori_loop(1, sp_count, greet_sp, 0)
    lax.fori_loop(1, members, greet_member, 0)
    def end_to(other):
        return pltpu.make_async_remote_copy(
            src_ref=end_ref,
            dst_ref=ends.at[sp],
            send_sem=end_send.at[other],
            recv_sem=end_recv.at[sp],
            device_id=(other, tp),
            device_id_type=MESH,
        )

    def end_from(other):
        return pltpu.make_async_remote_copy(
            src_ref=end_ref,
            dst_ref=ends.at[other],
            send_sem=end_send.at[other],
            recv_sem=end_recv.at[other],
            device_id=(other, tp),
            device_id_type=MESH,
        )

    def route_to(other):
        return pltpu.make_async_remote_copy(
            src_ref=routes_ref,
            dst_ref=all_routes.at[sp],
            send_sem=route_send.at[other],
            recv_sem=route_recv.at[sp],
            device_id=(other, tp),
            device_id_type=MESH,
        )

    def route_from(other):
        return pltpu.make_async_remote_copy(
            src_ref=routes_ref,
            dst_ref=all_routes.at[other],
            send_sem=route_send.at[other],
            recv_sem=route_recv.at[other],
            device_id=(other, tp),
            device_id_type=MESH,
        )

    def token_to(other):
        return pltpu.make_async_remote_copy(
            src_ref=mixed_ref.at[other],
            dst_ref=tokens.at[tp],
            send_sem=token_send.at[other],
            recv_sem=token_recv.at[tp],
            device_id=(sp, other),
            device_id_type=MESH,
        )

    def token_from(other):
        return pltpu.make_async_remote_copy(
            src_ref=mixed_ref.at[other],
            dst_ref=tokens.at[other],
            send_sem=token_send.at[other],
            recv_sem=token_recv.at[other],
            device_id=(sp, other),
            device_id_type=MESH,
        )

    def each_sp(action):
        def body(step, carry):
            action(lax.rem(sp + step, sp_count))
            return carry

        lax.fori_loop(1, sp_count, body, 0)

    def each_tp(action):
        def body(step, carry):
            action(lax.rem(tp + step, tp_count))
            return carry

        lax.fori_loop(1, tp_count, body, 0)

    for load in loads[:12]:
        load.wait()
    routes_ref[:top_count] = ids_ref[...].astype(jnp.float32)
    routes_ref[top_count:] = gates_ref[...]
    eye = lax.broadcasted_iota(jnp.int32, (groups, groups), 0) == lax.broadcasted_iota(
        jnp.int32, (groups, groups), 1
    )
    step_size = jnp.exp(jnp.sum(jnp.where(eye, step_ref[...], 0.0), axis=1, keepdims=True))
    decay_real = real_ref[...]
    decay_imag = imag_ref[...]
    magnitude = jnp.exp(decay_real * step_size)
    bar = (magnitude * jnp.cos(decay_imag * step_size), magnitude * jnp.sin(decay_imag * step_size))
    denominator = decay_real * decay_real + decay_imag * decay_imag
    less_one = bar[0] - 1.0
    coef = (
        ((less_one * decay_real + bar[1] * decay_imag) / denominator)[:, None, :],
        ((bar[1] * decay_real - less_one * decay_imag) / denominator)[:, None, :],
    )
    drive = times(coef, (in_re_ref[...], in_im_ref[...]))
    bar = tuple(flatten_rows(part, 8) for part in bar)
    spread = jnp.where(
        jnp.bitwise_and(lax.broadcasted_iota(jnp.int32, (states, wide), 1), states - 1)
        == lax.broadcasted_iota(jnp.int32, (states, wide), 0),
        1.0,
        0.0,
    ).astype(jnp.bfloat16)
    lane = lax.broadcasted_iota(jnp.int32, (channels, wide), 1)
    own = [
        jnp.logical_and(lane >= group * states, lane < (group + 1) * states) for group in range(groups)
    ]

    def scatter(table, target, part):
        for index, piece in enumerate(split_in_two(table.reshape(channel_count, states))):
            tiled = jnp.dot(piece, spread, preferred_element_type=jnp.float32)
            for group in range(groups):
                at = slice(group * channels, (group + 1) * channels)
                target[index, at, part * wide : (part + 1) * wide] = jnp.where(
                    own[group], tiled[at], 0.0
                ).astype(jnp.bfloat16)

    for part in range(2):
        scatter(drive[part], feeds, part)
    turn = jnp.where(
        lax.broadcasted_iota(jnp.int32, (states, states), 0)
        == lax.broadcasted_iota(jnp.int32, (states, states), 1),
        1.0,
        0.0,
    ).astype(jnp.bfloat16)
    across = (((1,), (1,)), ((), ()))
    channel = lax.broadcasted_iota(jnp.int32, (states, channel_count), 1)
    for part, table in enumerate((out_re_ref[...], -out_im_ref[...])):
        piece = table.reshape(channel_count, states).astype(jnp.bfloat16)
        turned = lax.dot_general(turn, piece, across, preferred_element_type=jnp.float32)
        for group in range(groups):
            here = jnp.logical_and(channel >= group * channels, channel < (group + 1) * channels)
            at = part * wide + group * states
            reads[at : at + states] = jnp.where(here, turned, 0.0).astype(jnp.bfloat16)

    order = lax.broadcasted_iota(jnp.int32, (length, length), 0)
    shuffle = jnp.where(
        lax.broadcasted_iota(jnp.int32, (length, length), 1)
        == jnp.bitwise_and(order, 7) * segment + lax.shift_right_logical(order, 3),
        1.0,
        0.0,
    ).astype(jnp.bfloat16)
    permuted[...] = jnp.dot(shuffle, inputs_ref[...], preferred_element_type=jnp.float32).astype(jnp.bfloat16)
    block = min(512, wide)
    for first in range(0, 2 * wide, block):
        states_ref[:, first : first + block] = jnp.dot(
            permuted[...], feeds[0, :, first : first + block], preferred_element_type=jnp.float32
        ) + jnp.dot(
            permuted[...], feeds[1, :, first : first + block], preferred_element_type=jnp.float32
        )

    def advance(start, keep):
        def body(index, state):
            at = pl.ds(pl.multiple_of(index * 8, 8), 8)
            moved = times(bar, state)
            state = (moved[0] + states_ref[at, :wide], moved[1] + states_ref[at, wide:])
            if keep:
                states_ref[at, :wide] = state[0]
                states_ref[at, wide:] = state[1]
            return state

        return lax.fori_loop(0, segment, body, start, unroll=4)

    zero = jnp.zeros((8, wide), jnp.float32)
    tails = advance((zero, zero), False)
    row = tuple(part[:1] for part in bar)
    power = 1
    while power < segment:
        row = times(row, row)
        power *= 2
    over_segment = row
    while power < length:
        row = times(row, row)
        power *= 2
    over_block = row
    nothing = (zero[:1], zero[:1])
    gathered = nothing
    for index in range(8):
        moved = times(over_segment, gathered)
        gathered = tuple(moved[part] + tails[part][index : index + 1] for part in range(2))
    end_ref[0:1] = gathered[0]
    end_ref[1:2] = gathered[1]
    pl.semaphore_wait(barrier, sp_count - 1 + members - 1)
    each_sp(lambda other: end_to(other).start())
    each_sp(lambda other: route_to(other).start())
    all_routes[sp] = routes_ref[...]
    each_sp(lambda other: end_from(other).wait_recv())
    carried = nothing
    for source in range(sp_count):
        moved = times(over_block, carried)
        earlier = sp > source
        carried = tuple(
            jnp.where(earlier, moved[part] + ends[source, part : part + 1], carried[part]) for part in range(2)
        )
    begins = ([], [])
    for index in range(8):
        for part in range(2):
            begins[part].append(carried[part])
        moved = times(over_segment, carried)
        carried = tuple(moved[part] + tails[part][index : index + 1] for part in range(2))
    advance(tuple(jnp.concatenate(part, axis=0) for part in begins), True)

    gains = flatten_rows(skip_ref[...], 1)
    mixed = []
    for first in range(0, length, rows):
        readout = jnp.dot(
            states_ref[first : first + rows].astype(jnp.bfloat16),
            reads[...],
            preferred_element_type=jnp.float32,
        )
        direct = gains * permuted[first : first + rows].astype(jnp.float32)
        mixed.append(jax.nn.gelu(readout + direct).astype(jnp.bfloat16))
    mixed = jnp.concatenate(mixed, axis=0)
    ordered = lax.dot_general(
        shuffle, mixed, (((0,), (0,)), ((), ())), preferred_element_type=jnp.float32
    ).astype(jnp.bfloat16)
    for other in range(tp_count):
        mixed_ref[other] = ordered[other * rows : (other + 1) * rows]
    each_tp(lambda other: token_to(other).start())
    tokens[tp] = mixed_ref[tp]
    visits = visiting_order(planes)

    def visited(step):
        block = jnp.int32(visits[0][step])
        for own in range(1, planes):
            block = jnp.where(plane == own, visits[own][step], block)
        return block

    steps = [plane] + [visited(step) for step in range(1, planes)]

    def pass_up(block, part):
        return pltpu.make_async_remote_copy(
            src_ref=blocks.at[block * SPLIT + part],
            dst_ref=blocks.at[block * SPLIT + part],
            send_sem=up_sem.at[block * SPLIT + part],
            recv_sem=block_sem.at[block * SPLIT + part],
            device_id=plane_id(jnp.minimum(plane + 1, planes - 1)),
            device_id_type=MESH,
        )

    def pass_down(block, part):
        return pltpu.make_async_remote_copy(
            src_ref=blocks.at[block * SPLIT + part],
            dst_ref=blocks.at[block * SPLIT + part],
            send_sem=down_sem.at[block * SPLIT + part],
            recv_sem=block_sem.at[block * SPLIT + part],
            device_id=plane_id(jnp.maximum(plane - 1, 0)),
            device_id_type=MESH,
        )

    def goes_up(block):
        return jnp.logical_and(block <= plane, plane < planes - 1)

    def goes_down(block):
        return jnp.logical_and(block >= plane, plane > 0)

    def forward(block, part):
        @pl.when(goes_up(block))
        def _():
            pass_up(block, part).start()

        @pl.when(goes_down(block))
        def _():
            pass_down(block, part).start()

    def deal(block, other):
        return pltpu.make_async_remote_copy(
            src_ref=sent.at[block, other],
            dst_ref=arrived.at[block, me],
            send_sem=sent_sem.at[block, other],
            recv_sem=arrived_sem.at[block, me],
            device_id=member_id(other),
            device_id_type=MESH,
        )

    def reply(block, other):
        return pltpu.make_async_remote_copy(
            src_ref=replies.at[block, other],
            dst_ref=returned.at[block, me],
            send_sem=replies_sem.at[block, other],
            recv_sem=returned_sem.at[block, me],
            device_id=member_id(other),
            device_id_type=MESH,
        )

    def landing(buffer, sem, block, other):
        return pltpu.make_async_remote_copy(
            src_ref=buffer.at[block, other],
            dst_ref=buffer.at[block, other],
            send_sem=sem.at[block, other],
            recv_sem=sem.at[block, other],
            device_id=member_id(other),
            device_id_type=MESH,
        )

    def homeward(block, part):
        return pltpu.make_async_remote_copy(
            src_ref=partial.at[block * SHARE + part],
            dst_ref=homed.at[plane * SHARE + part],
            send_sem=partial_sem.at[block * SHARE + part],
            recv_sem=homed_sem.at[plane * SHARE + part],
            device_id=plane_id(block),
            device_id_type=MESH,
        )

    joins = planes == 4
    inner = jnp.logical_and(plane > 0, plane < planes - 1)
    beside = plane + 1 - 2 * lax.rem(plane, 2)

    def join(block, step, part):
        slot = (step - 2) * SHARE + part
        return pltpu.make_async_remote_copy(
            src_ref=partial.at[block * SHARE + part],
            dst_ref=joined.at[slot],
            send_sem=partial_sem.at[block * SHARE + part],
            recv_sem=joined_sem.at[slot],
            device_id=plane_id(beside),
            device_id_type=MESH,
        )

    def each_other(action):
        def body(step, carry):
            action(lax.rem(me + step, members))
            return carry

        lax.fori_loop(1, members, body, 0)

    def place(block):
        routes = all_routes[block * rows_y + row_y]
        experts = (lax.broadcasted_iota(jnp.int32, (members, row_count), 0) + plane * members).astype(
            jnp.float32
        )
        named = jnp.zeros((members, row_count), jnp.float32)
        gates = jnp.zeros((members, row_count), jnp.float32)
        for index in range(top_count):
            hit = experts == routes[index : index + 1, :]
            named = named + jnp.where(hit, 1.0, 0.0)
            gates = gates + jnp.where(hit, routes[top_count + index : top_count + index + 1, :], 0.0)
        before = (
            lax.broadcasted_iota(jnp.int32, (row_count, row_count), 0)
            < lax.broadcasted_iota(jnp.int32, (row_count, row_count), 1)
        )
        ranks = jnp.dot(
            named.astype(jnp.bfloat16),
            jnp.where(before, 1.0, 0.0).astype(jnp.bfloat16),
            preferred_element_type=jnp.float32,
        )
        ranks = jnp.where(named > 0.5, ranks, -1.0)
        numbers = lax.broadcasted_iota(jnp.int32, (capacity, row_count), 0).astype(jnp.float32)
        hits = [ranks[other : other + 1, :] == numbers for other in range(members)]
        picked = jnp.concatenate([jnp.where(hit, 1.0, 0.0) for hit in hits], axis=0)
        scaled = jnp.concatenate(
            [jnp.where(hits[other], gates[other : other + 1, :], 0.0) for other in range(members)], axis=0
        )
        coarse = scaled.astype(jnp.bfloat16)
        mix_weights[block, :, :row_count] = coarse
        mix_weights[block, :, row_count:] = (scaled - coarse.astype(jnp.float32)).astype(jnp.bfloat16)
        picks[block] = picked.astype(jnp.bfloat16)

    def relay(step, part):
        pass_up(steps[step], part).wait_recv()
        forward(steps[step], part)

    def dispatch(step, part):
        block = steps[step]
        slab = block * SPLIT + part
        picked = picks[block]
        for first in range(0, part_width, column):
            rows = jnp.dot(
                picked, blocks[slab, :, first : first + column], preferred_element_type=jnp.float32
            )
            for other in range(members):
                sent[slab, other, :, first : first + column] = rows[
                    other * capacity : (other + 1) * capacity
                ].astype(jnp.bfloat16)
        each_other(lambda other: deal(slab, other).start())
        arrived[slab, me] = sent[slab, me]

    def apply_expert(step, part):
        block = steps[step]
        for piece in range(SPLIT):
            slab = block * SPLIT + piece
            each_other(lambda other: landing(arrived, arrived_sem, slab, other).wait_recv())
            for other in range(members):
                wide_rows[
                    other * capacity : (other + 1) * capacity, piece * part_width : (piece + 1) * part_width
                ] = arrived[slab, other].astype(jnp.float32)
        rows = wide_rows[...].astype(jnp.bfloat16)
        gate = jnp.dot(rows, gate_w[0], preferred_element_type=jnp.float32)
        up = jnp.dot(rows, up_w[0], preferred_element_type=jnp.float32)
        hidden = (jax.nn.silu(gate) * up).astype(jnp.bfloat16)
        for piece in range(SHARE):
            slab = block * SHARE + piece
            for first in range(0, share_width, column):
                at = piece * share_width + first
                rows = jnp.dot(hidden, down_w[0, :, at : at + column], preferred_element_type=jnp.float32)
                for other in range(members):
                    replies[slab, other, :, first : first + column] = rows[
                        other * capacity : (other + 1) * capacity
                    ].astype(jnp.bfloat16)
            each_other(lambda other: reply(slab, other).start())
            returned[slab, me] = replies[slab, me]

    def combine(step, part):
        block = steps[step]
        slab = block * SHARE + part
        each_other(lambda other: landing(returned, returned_sem, slab, other).wait_recv())
        weights = mix_weights[block]
        for first in range(0, share_width, column):
            rows = jnp.concatenate(
                [returned[slab, other, :, first : first + column].astype(jnp.float32) for other in range(members)],
                axis=0,
            ).astype(jnp.bfloat16)
            both = lax.dot_general(
                weights, rows, (((0,), (0,)), ((), ())), preferred_element_type=jnp.float32
            )
            added = both[:row_count] + both[row_count:]
            if step == 0:
                at = part * share_width + first
                total[:, at : at + column] += added
            else:
                partial[slab, :, first : first + column] = added.astype(jnp.bfloat16)
                if joins and step > 1:
                    kept[(step - 2) * SHARE + part, :, first : first + column] = added
        if joins and step > 1:

            @pl.when(jnp.logical_not(inner))
            def _():
                join(block, step, part).start()

        elif step > 0:
            homeward(block, part).start()

    def merge(step, part):
        block = steps[step]
        slot = (step - 2) * SHARE + part

        @pl.when(inner)
        def _():
            join(block, step, part).wait_recv()
            partial[block * SHARE + part] = (kept[slot] + joined[slot].astype(jnp.float32)).astype(jnp.bfloat16)
            homeward(block, part).start()

    def shared(step, part):
        rows = hidden_ref[...]
        gate = jnp.dot(rows, sgate_w[...], preferred_element_type=jnp.float32)
        up = jnp.dot(rows, sup_w[...], preferred_element_type=jnp.float32)
        hidden = (jax.nn.silu(gate) * up).astype(jnp.bfloat16)
        for first in range(0, width, column):
            total[:, first : first + column] += jnp.dot(
                hidden, sdown_w[:, first : first + column], preferred_element_type=jnp.float32
            )

    each_sp(lambda other: route_from(other).wait_recv())
    for block in range(planes):
        place(block)
    for load in loads[12:17]:
        load.wait()
    each_tp(lambda other: token_from(other).wait_recv())
    token_rows = jnp.concatenate([tokens[other] for other in range(tp_count)], axis=1)
    pre_gate = jnp.dot(token_rows, glu_w[...], preferred_element_type=jnp.float32) + bias_ref[...]
    gated = token_rows.astype(jnp.float32) * jax.nn.sigmoid(pre_gate)
    normed = rms_scale(gated, mix_gain_ref[...]).astype(jnp.bfloat16)
    stream = residual_ref[...].astype(jnp.float32) + jnp.dot(
        normed, proj_w[...], preferred_element_type=jnp.float32
    )
    total[...] = stream
    hidden = rms_scale(stream, norm_gain_ref[...]).astype(jnp.bfloat16)
    hidden_ref[...] = hidden
    for part in range(SPLIT):
        blocks[plane * SPLIT + part] = hidden[:, part * part_width : (part + 1) * part_width]
        forward(plane, part)
    for load in loads[17:]:
        load.wait()
    actions = {"A": dispatch, "F": relay, "S": shared, "B": apply_expert, "C": combine, "M": merge}
    for stage, step, part in stages_of(planes):
        actions[stage](step, part)
    senders = [beside, jnp.where(plane < 2, 2, 1)] if joins else steps[1:]
    for part in range(SHARE):
        at = slice(part * share_width, (part + 1) * share_width)
        result = total[:, at]
        for source in senders:
            pltpu.make_async_remote_copy(
                src_ref=partial.at[source * SHARE + part],
                dst_ref=homed.at[source * SHARE + part],
                send_sem=partial_sem.at[source * SHARE + part],
                recv_sem=homed_sem.at[source * SHARE + part],
                device_id=plane_id(source),
                device_id_type=MESH,
            ).wait_recv()
            result = result + homed[source * SHARE + part].astype(jnp.float32)
        out_ref[:, at] = result.astype(out_ref.dtype)

    for step in range(planes):
        block = steps[step]
        for part in range(SPLIT):

            @pl.when(goes_up(block))
            def _():
                pass_up(block, part).wait_send()

            @pl.when(goes_down(block))
            def _():
                pass_down(block, part).wait_send()

            each_other(lambda other: deal(block * SPLIT + part, other).wait_send())
        for part in range(SHARE):
            each_other(lambda other: reply(block * SHARE + part, other).wait_send())
            if step > 0:
                homeward(block, part).wait_send()
    each_sp(lambda other: end_to(other).wait_send())
    each_sp(lambda other: route_to(other).wait_send())
    each_tp(lambda other: token_to(other).wait_send())


def layer(arguments, capacity, collective_id):
    sp_count, tp_count = lax.axis_size("sp"), lax.axis_size("tp")
    inputs, residual, input_re = arguments[0], arguments[1], arguments[5]
    length, channel_count = inputs.shape
    groups, channels, states = input_re.shape
    rows, width = residual.shape
    top_count = arguments[10].shape[0]
    wide = groups * states
    planes = planes_of(sp_count)
    members = sp_count * tp_count // planes
    capacity = -(-capacity // 8) * 8
    slots = members * capacity
    hbm = pl.BlockSpec(memory_space=pl.ANY)
    bf16, f32 = jnp.bfloat16, jnp.float32
    vmem, dma = pltpu.VMEM, pltpu.SemaphoreType.DMA
    pieces = vmem((planes * SPLIT, members, capacity, width // SPLIT), bf16)
    shares = vmem((planes * SHARE, members, capacity, width // SHARE), bf16)
    whole = vmem((planes * SPLIT, rows, width // SPLIT), bf16)
    parts = vmem((planes * SHARE, rows, width // SHARE), bf16)
    tables = vmem((2, channel_count, 2 * wide), bf16)
    tokens = vmem((tp_count, rows, channel_count), bf16)
    routes = (2 * top_count, rows)
    return pl.pallas_call(
        functools.partial(layer_kernel, sp_count, tp_count, capacity),
        out_shape=jax.ShapeDtypeStruct((rows, width), bf16),
        in_specs=[hbm] * len(arguments),
        out_specs=pl.BlockSpec(memory_space=pltpu.VMEM),
        scratch_shapes=[vmem(argument.shape, argument.dtype) for argument in arguments]
        + [
            tables,
            vmem((2 * wide, channel_count), bf16),
            vmem((length, 2 * wide), f32),
            vmem((length, channel_count), bf16),
            tokens,
            vmem((2, wide), f32),
            vmem((sp_count, 2, wide), f32),
            tokens,
            vmem(routes, f32),
            vmem((sp_count,) + routes, f32),
            vmem((planes, slots, rows), bf16),
            vmem((rows, width), bf16),
            whole,
            pieces,
            pieces,
            shares,
            shares,
            parts,
            parts,
            vmem((planes, slots, 2 * rows), bf16),
            vmem((2 * SHARE, rows, width // SHARE), f32),
            vmem((2 * SHARE, rows, width // SHARE), bf16),
            vmem((slots, width), f32),
            vmem((rows, width), f32),
            dma((len(arguments),)),
        ]
        + [dma((sp_count,))] * 4
        + [dma((tp_count,))] * 2
        + [dma((planes * SPLIT,))] * 3
        + [dma((planes * SPLIT, members))] * 2
        + [dma((planes * SHARE, members))] * 2
        + [dma((planes * SHARE,))] * 2
        + [dma((2 * SHARE,))],
        compiler_params=pltpu.CompilerParams(
            collective_id=collective_id, has_side_effects=True, vmem_limit_bytes=63 * 2**20
        ),
    )(*arguments)


def on_device(
    mixer_input,
    residual,
    decay_real,
    decay_imag,
    log_step,
    input_re,
    input_im,
    output_re,
    output_im,
    skip_gain,
    glu_weight,
    glu_bias,
    mix_gain,
    out_weight,
    norm_gain,
    route_ids,
    route_gates,
    expert_gate,
    expert_up,
    expert_down,
    shared_gate,
    shared_up,
    shared_down,
):
    row_count, top_count = route_ids.shape
    expert_count = lax.axis_size(("sp", "tp"))
    capacity = max(2, 3 * row_count * top_count // (2 * expert_count))
    arguments = (
        mixer_input,
        residual,
        decay_real,
        decay_imag,
        log_step[None, :],
        jnp.swapaxes(input_re, 1, 2),
        jnp.swapaxes(input_im, 1, 2),
        output_re,
        output_im,
        skip_gain,
        route_ids.T,
        route_gates.T,
        glu_weight,
        glu_bias[None, :],
        mix_gain[None, :],
        out_weight,
        norm_gain[None, :],
        shared_gate,
        shared_up,
        shared_down,
        expert_gate,
        expert_up,
        expert_down,
    )
    return layer(arguments, capacity, 1)


def solution(mesh):
    return jax.shard_map(
        on_device,
        mesh=mesh,
        in_specs=(
            P("sp", "tp"),
            P(("sp", "tp"), None),
            P("tp", None),
            P("tp", None),
            P("tp"),
            P("tp", None, None),
            P("tp", None, None),
            P("tp", None, None),
            P("tp", None, None),
            P("tp", None),
            P(),
            P(),
            P(),
            P(),
            P(),
            P(("sp", "tp"), None),
            P(("sp", "tp"), None),
            P(("sp", "tp"), None, None),
            P(("sp", "tp"), None, None),
            P(("sp", "tp"), None, None),
            P(),
            P(),
            P(),
        ),
        out_specs=P(("sp", "tp"), None),
        check_vma=False,
    )
```

```python
import functools
import math

import jax
import jax.numpy as jnp
from jax import lax
from jax.experimental import pallas as pl
from jax.experimental.pallas import tpu as pltpu
from jax.sharding import PartitionSpec as P

NORM_EPS = 1e-06
HIGHEST = lax.Precision.HIGHEST
MESH = pl.DeviceIdType.MESH


def times(a, b):
    return (a[0] * b[0] - a[1] * b[1], a[0] * b[1] + a[1] * b[0])


def rms_scale(values, gain):
    return values * lax.rsqrt(jnp.mean(values * values, axis=-1, keepdims=True) + NORM_EPS) * gain


def flatten_rows(values, count):
    groups, states = values.shape
    width = groups * states
    lanes = lax.broadcasted_iota(jnp.int32, (states, width), 1)
    spread = jnp.where(
        jnp.bitwise_and(lanes, states - 1) == lax.broadcasted_iota(jnp.int32, (states, width), 0), 1.0, 0.0
    )
    tiled = jnp.dot(values, spread, precision=HIGHEST, preferred_element_type=jnp.float32)
    first = lax.broadcasted_iota(jnp.int32, (groups, width), 0) * states
    lanes = lax.broadcasted_iota(jnp.int32, (groups, width), 1)
    own = jnp.logical_and(lanes >= first, lanes < first + states)
    row = jnp.sum(jnp.where(own, tiled, 0.0), axis=0, keepdims=True)
    return jnp.broadcast_to(row, (count, width))


def split_in_two(values):
    coarse = values.astype(jnp.bfloat16)
    return coarse, (values - coarse.astype(jnp.float32)).astype(jnp.bfloat16)


SPLIT = 2
SHARE = 2
STAGES = (
    "A00S00A01F10A10F20A20F11A11F21A21F30A30F31",
    "A31B20B30C20B10C21C30B00C31M20C10M21C11M30",
    "C00C01M31",
)


def stages_of(planes):
    if planes == 4:
        return [
            (text[at], int(text[at + 1]), int(text[at + 2])) for text in STAGES for at in range(0, len(text), 3)
        ]
    stages = [("A", 0, part) for part in range(SPLIT)] + [("S", 0, 0)]
    for step in range(1, planes):
        stages += [(stage, step, part) for part in range(SPLIT) for stage in "FA"]
        stages += [("B", step, 0)] + [("C", step, part) for part in range(SHARE)]
    return stages + [("B", 0, 0)] + [("C", 0, part) for part in range(SHARE)]


def planes_of(sp_count):
    return math.gcd(sp_count, 4)


def visiting_order(planes):
    if planes == 4:
        return [[0, 1, 2, 3], [1, 0, 2, 3], [2, 3, 1, 0], [3, 2, 1, 0]]
    return [sorted(range(planes), key=lambda other: (abs(other - own), -other)) for own in range(planes)]


def layer_kernel(
    sp_count,
    tp_count,
    capacity,
    *refs,
):
    sources = refs[:23]
    out_ref = refs[23]
    held = refs[24:47]
    (
        inputs_ref,
        residual_ref,
        real_ref,
        imag_ref,
        step_ref,
        in_re_ref,
        in_im_ref,
        out_re_ref,
        out_im_ref,
        skip_ref,
        ids_ref,
        gates_ref,
        glu_w,
        bias_ref,
        mix_gain_ref,
        proj_w,
        norm_gain_ref,
        sgate_w,
        sup_w,
        sdown_w,
        gate_w,
        up_w,
        down_w,
    ) = held
    (
        feeds,
        reads,
        states_ref,
        permuted,
        mixed_ref,
        end_ref,
        ends,
        tokens,
        routes_ref,
        all_routes,
        picks,
        hidden_ref,
        blocks,
        sent,
        arrived,
        replies,
        returned,
        partial,
        homed,
        mix_weights,
        kept,
        joined,
        wide_rows,
        total,
        load_sem,
        end_send,
        end_recv,
        route_send,
        route_recv,
        token_send,
        token_recv,
        up_sem,
        down_sem,
        block_sem,
        sent_sem,
        arrived_sem,
        replies_sem,
        returned_sem,
        partial_sem,
        homed_sem,
        joined_sem,
    ) = refs[47:]
    sp = lax.axis_index("sp")
    tp = lax.axis_index("tp")
    length, channel_count = inputs_ref.shape
    groups, channels, states = in_re_ref.shape
    wide = groups * states
    segment = length // 8
    rows = length // tp_count
    planes = planes_of(sp_count)
    rows_y = sp_count // planes
    members = rows_y * tp_count
    width = residual_ref.shape[1]
    row_count = rows
    top_count = ids_ref.shape[0]
    part_width = width // SPLIT
    share_width = width // SHARE
    column = min(512, part_width, share_width)
    plane = sp // rows_y
    row_y = lax.rem(sp, rows_y)
    me = row_y * tp_count + tp

    barrier = pltpu.get_barrier_semaphore()

    def greet_sp(step, carry):
        pl.semaphore_signal(
            barrier, inc=1, device_id=(lax.rem(sp + step, sp_count), tp), device_id_type=MESH
        )
        return carry

    def member_id(other):
        return (plane * rows_y + other // tp_count, lax.rem(other, tp_count))

    def plane_id(other):
        return (other * rows_y + row_y, tp)

    def greet_member(step, carry):
        pl.semaphore_signal(
            barrier, inc=1, device_id=member_id(lax.rem(me + step, members)), device_id_type=MESH
        )
        return carry

    loads = [
        pltpu.make_async_copy(source, target, load_sem.at[number])
        for number, (source, target) in enumerate(zip(sources, held))
    ]
    for load in loads:
        load.start()
    lax.fori_loop(1, sp_count, greet_sp, 0)
    lax.fori_loop(1, members, greet_member, 0)
    def end_to(other):
        return pltpu.make_async_remote_copy(
            src_ref=end_ref,
            dst_ref=ends.at[sp],
            send_sem=end_send.at[other],
            recv_sem=end_recv.at[sp],
            device_id=(other, tp),
            device_id_type=MESH,
        )

    def end_from(other):
        return pltpu.make_async_remote_copy(
            src_ref=end_ref,
            dst_ref=ends.at[other],
            send_sem=end_send.at[other],
            recv_sem=end_recv.at[other],
            device_id=(other, tp),
            device_id_type=MESH,
        )

    def route_to(other):
        return pltpu.make_async_remote_copy(
            src_ref=routes_ref,
            dst_ref=all_routes.at[sp],
            send_sem=route_send.at[other],
            recv_sem=route_recv.at[sp],
            device_id=(other, tp),
            device_id_type=MESH,
        )

    def route_from(other):
        return pltpu.make_async_remote_copy(
            src_ref=routes_ref,
            dst_ref=all_routes.at[other],
            send_sem=route_send.at[other],
            recv_sem=route_recv.at[other],
            device_id=(other, tp),
            device_id_type=MESH,
        )

    def token_to(other):
        return pltpu.make_async_remote_copy(
            src_ref=mixed_ref.at[other],
            dst_ref=tokens.at[tp],
            send_sem=token_send.at[other],
            recv_sem=token_recv.at[tp],
            device_id=(sp, other),
            device_id_type=MESH,
        )

    def token_from(other):
        return pltpu.make_async_remote_copy(
            src_ref=mixed_ref.at[other],
            dst_ref=tokens.at[other],
            send_sem=token_send.at[other],
            recv_sem=token_recv.at[other],
            device_id=(sp, other),
            device_id_type=MESH,
        )

    def each_sp(action):
        def body(step, carry):
            action(lax.rem(sp + step, sp_count))
            return carry

        lax.fori_loop(1, sp_count, body, 0)

    def each_tp(action):
        def body(step, carry):
            action(lax.rem(tp + step, tp_count))
            return carry

        lax.fori_loop(1, tp_count, body, 0)

    for load in loads[:12]:
        load.wait()
    routes_ref[:top_count] = ids_ref[...].astype(jnp.float32)
    routes_ref[top_count:] = gates_ref[...]
    eye = lax.broadcasted_iota(jnp.int32, (groups, groups), 0) == lax.broadcasted_iota(
        jnp.int32, (groups, groups), 1
    )
    step_size = jnp.exp(jnp.sum(jnp.where(eye, step_ref[...], 0.0), axis=1, keepdims=True))
    decay_real = real_ref[...]
    decay_imag = imag_ref[...]
    magnitude = jnp.exp(decay_real * step_size)
    bar = (magnitude * jnp.cos(decay_imag * step_size), magnitude * jnp.sin(decay_imag * step_size))
    denominator = decay_real * decay_real + decay_imag * decay_imag
    less_one = bar[0] - 1.0
    coef = (
        ((less_one * decay_real + bar[1] * decay_imag) / denominator)[:, None, :],
        ((bar[1] * decay_real - less_one * decay_imag) / denominator)[:, None, :],
    )
    drive = times(coef, (in_re_ref[...], in_im_ref[...]))
    bar = tuple(flatten_rows(part, 8) for part in bar)
    spread = jnp.where(
        jnp.bitwise_and(lax.broadcasted_iota(jnp.int32, (states, wide), 1), states - 1)
        == lax.broadcasted_iota(jnp.int32, (states, wide), 0),
        1.0,
        0.0,
    ).astype(jnp.bfloat16)
    lane = lax.broadcasted_iota(jnp.int32, (channels, wide), 1)
    own = [
        jnp.logical_and(lane >= group * states, lane < (group + 1) * states) for group in range(groups)
    ]

    def scatter(table, target, part):
        for index, piece in enumerate(split_in_two(table.reshape(channel_count, states))):
            tiled = jnp.dot(piece, spread, preferred_element_type=jnp.float32)
            for group in range(groups):
                at = slice(group * channels, (group + 1) * channels)
                target[index, at, part * wide : (part + 1) * wide] = jnp.where(
                    own[group], tiled[at], 0.0
                ).astype(jnp.bfloat16)

    for part in range(2):
        scatter(drive[part], feeds, part)
    turn = jnp.where(
        lax.broadcasted_iota(jnp.int32, (states, states), 0)
        == lax.broadcasted_iota(jnp.int32, (states, states), 1),
        1.0,
        0.0,
    ).astype(jnp.bfloat16)
    across = (((1,), (1,)), ((), ()))
    channel = lax.broadcasted_iota(jnp.int32, (states, channel_count), 1)
    for part, table in enumerate((out_re_ref[...], -out_im_ref[...])):
        piece = table.reshape(channel_count, states).astype(jnp.bfloat16)
        turned = lax.dot_general(turn, piece, across, preferred_element_type=jnp.float32)
        for group in range(groups):
            here = jnp.logical_and(channel >= group * channels, channel < (group + 1) * channels)
            at = part * wide + group * states
            reads[at : at + states] = jnp.where(here, turned, 0.0).astype(jnp.bfloat16)

    order = lax.broadcasted_iota(jnp.int32, (length, length), 0)
    shuffle = jnp.where(
        lax.broadcasted_iota(jnp.int32, (length, length), 1)
        == jnp.bitwise_and(order, 7) * segment + lax.shift_right_logical(order, 3),
        1.0,
        0.0,
    ).astype(jnp.bfloat16)
    permuted[...] = jnp.dot(shuffle, inputs_ref[...], preferred_element_type=jnp.float32).astype(jnp.bfloat16)
    block = min(512, wide)
    for first in range(0, 2 * wide, block):
        states_ref[:, first : first + block] = jnp.dot(
            permuted[...], feeds[0, :, first : first + block], preferred_element_type=jnp.float32
        ) + jnp.dot(
            permuted[...], feeds[1, :, first : first + block], preferred_element_type=jnp.float32
        )

    def advance(start, keep):
        def body(index, state):
            at = pl.ds(pl.multiple_of(index * 8, 8), 8)
            moved = times(bar, state)
            state = (moved[0] + states_ref[at, :wide], moved[1] + states_ref[at, wide:])
            if keep:
                states_ref[at, :wide] = state[0]
                states_ref[at, wide:] = state[1]
            return state

        return lax.fori_loop(0, segment, body, start, unroll=4)

    zero = jnp.zeros((8, wide), jnp.float32)
    tails = advance((zero, zero), False)
    row = tuple(part[:1] for part in bar)
    power = 1
    while power < segment:
        row = times(row, row)
        power *= 2
    over_segment = row
    while power < length:
        row = times(row, row)
        power *= 2
    over_block = row
    nothing = (zero[:1], zero[:1])
    gathered = nothing
    for index in range(8):
        moved = times(over_segment, gathered)
        gathered = tuple(moved[part] + tails[part][index : index + 1] for part in range(2))
    end_ref[0:1] = gathered[0]
    end_ref[1:2] = gathered[1]
    pl.semaphore_wait(barrier, sp_count - 1 + members - 1)
    each_sp(lambda other: end_to(other).start())
    each_sp(lambda other: route_to(other).start())
    all_routes[sp] = routes_ref[...]
    each_sp(lambda other: end_from(other).wait_recv())
    carried = nothing
    for source in range(sp_count):
        moved = times(over_block, carried)
        earlier = sp > source
        carried = tuple(
            jnp.where(earlier, moved[part] + ends[source, part : part + 1], carried[part]) for part in range(2)
        )
    begins = ([], [])
    for index in range(8):
        for part in range(2):
            begins[part].append(carried[part])
        moved = times(over_segment, carried)
        carried = tuple(moved[part] + tails[part][index : index + 1] for part in range(2))
    advance(tuple(jnp.concatenate(part, axis=0) for part in begins), True)

    gains = flatten_rows(skip_ref[...], 1)
    mixed = []
    for first in range(0, length, rows):
        readout = jnp.dot(
            states_ref[first : first + rows].astype(jnp.bfloat16),
            reads[...],
            preferred_element_type=jnp.float32,
        )
        direct = gains * permuted[first : first + rows].astype(jnp.float32)
        mixed.append(jax.nn.gelu(readout + direct).astype(jnp.bfloat16))
    mixed = jnp.concatenate(mixed, axis=0)
    ordered = lax.dot_general(
        shuffle, mixed, (((0,), (0,)), ((), ())), preferred_element_type=jnp.float32
    ).astype(jnp.bfloat16)
    for other in range(tp_count):
        mixed_ref[other] = ordered[other * rows : (other + 1) * rows]
    each_tp(lambda other: token_to(other).start())
    tokens[tp] = mixed_ref[tp]
    visits = visiting_order(planes)

    def visited(step):
        block = jnp.int32(visits[0][step])
        for own in range(1, planes):
            block = jnp.where(plane == own, visits[own][step], block)
        return block

    steps = [plane] + [visited(step) for step in range(1, planes)]

    def pass_up(block, part):
        return pltpu.make_async_remote_copy(
            src_ref=blocks.at[block * SPLIT + part],
            dst_ref=blocks.at[block * SPLIT + part],
            send_sem=up_sem.at[block * SPLIT + part],
            recv_sem=block_sem.at[block * SPLIT + part],
            device_id=plane_id(jnp.minimum(plane + 1, planes - 1)),
            device_id_type=MESH,
        )

    def pass_down(block, part):
        return pltpu.make_async_remote_copy(
            src_ref=blocks.at[block * SPLIT + part],
            dst_ref=blocks.at[block * SPLIT + part],
            send_sem=down_sem.at[block * SPLIT + part],
            recv_sem=block_sem.at[block * SPLIT + part],
            device_id=plane_id(jnp.maximum(plane - 1, 0)),
            device_id_type=MESH,
        )

    def goes_up(block):
        return jnp.logical_and(block <= plane, plane < planes - 1)

    def goes_down(block):
        return jnp.logical_and(block >= plane, plane > 0)

    def forward(block, part):
        @pl.when(goes_up(block))
        def _():
            pass_up(block, part).start()

        @pl.when(goes_down(block))
        def _():
            pass_down(block, part).start()

    def deal(block, other):
        return pltpu.make_async_remote_copy(
            src_ref=sent.at[block, other],
            dst_ref=arrived.at[block, me],
            send_sem=sent_sem.at[block, other],
            recv_sem=arrived_sem.at[block, me],
            device_id=member_id(other),
            device_id_type=MESH,
        )

    def reply(block, other):
        return pltpu.make_async_remote_copy(
            src_ref=replies.at[block, other],
            dst_ref=returned.at[block, me],
            send_sem=replies_sem.at[block, other],
            recv_sem=returned_sem.at[block, me],
            device_id=member_id(other),
            device_id_type=MESH,
        )

    def landing(buffer, sem, block, other):
        return pltpu.make_async_remote_copy(
            src_ref=buffer.at[block, other],
            dst_ref=buffer.at[block, other],
            send_sem=sem.at[block, other],
            recv_sem=sem.at[block, other],
            device_id=member_id(other),
            device_id_type=MESH,
        )

    def homeward(block, part):
        return pltpu.make_async_remote_copy(
            src_ref=partial.at[block * SHARE + part],
            dst_ref=homed.at[plane * SHARE + part],
            send_sem=partial_sem.at[block * SHARE + part],
            recv_sem=homed_sem.at[plane * SHARE + part],
            device_id=plane_id(block),
            device_id_type=MESH,
        )

    joins = planes == 4
    inner = jnp.logical_and(plane > 0, plane < planes - 1)
    beside = plane + 1 - 2 * lax.rem(plane, 2)

    def join(block, step, part):
        slot = (step - 2) * SHARE + part
        return pltpu.make_async_remote_copy(
            src_ref=partial.at[block * SHARE + part],
            dst_ref=joined.at[slot],
            send_sem=partial_sem.at[block * SHARE + part],
            recv_sem=joined_sem.at[slot],
            device_id=plane_id(beside),
            device_id_type=MESH,
        )

    def each_other(action):
        def body(step, carry):
            action(lax.rem(me + step, members))
            return carry

        lax.fori_loop(1, members, body, 0)

    def place(block):
        routes = all_routes[block * rows_y + row_y]
        experts = (lax.broadcasted_iota(jnp.int32, (members, row_count), 0) + plane * members).astype(
            jnp.float32
        )
        named = jnp.zeros((members, row_count), jnp.float32)
        gates = jnp.zeros((members, row_count), jnp.float32)
        for index in range(top_count):
            hit = experts == routes[index : index + 1, :]
            named = named + jnp.where(hit, 1.0, 0.0)
            gates = gates + jnp.where(hit, routes[top_count + index : top_count + index + 1, :], 0.0)
        before = (
            lax.broadcasted_iota(jnp.int32, (row_count, row_count), 0)
            < lax.broadcasted_iota(jnp.int32, (row_count, row_count), 1)
        )
        ranks = jnp.dot(
            named.astype(jnp.bfloat16),
            jnp.where(before, 1.0, 0.0).astype(jnp.bfloat16),
            preferred_element_type=jnp.float32,
        )
        ranks = jnp.where(named > 0.5, ranks, -1.0)
        numbers = lax.broadcasted_iota(jnp.int32, (capacity, row_count), 0).astype(jnp.float32)
        hits = [ranks[other : other + 1, :] == numbers for other in range(members)]
        picked = jnp.concatenate([jnp.where(hit, 1.0, 0.0) for hit in hits], axis=0)
        scaled = jnp.concatenate(
            [jnp.where(hits[other], gates[other : other + 1, :], 0.0) for other in range(members)], axis=0
        )
        coarse = scaled.astype(jnp.bfloat16)
        mix_weights[block, :, :row_count] = coarse
        mix_weights[block, :, row_count:] = (scaled - coarse.astype(jnp.float32)).astype(jnp.bfloat16)
        picks[block] = picked.astype(jnp.bfloat16)

    def relay(step, part):
        pass_up(steps[step], part).wait_recv()
        forward(steps[step], part)

    def dispatch(step, part):
        block = steps[step]
        slab = block * SPLIT + part
        picked = picks[block]
        for first in range(0, part_width, column):
            rows = jnp.dot(
                picked, blocks[slab, :, first : first + column], preferred_element_type=jnp.float32
            )
            for other in range(members):
                sent[slab, other, :, first : first + column] = rows[
                    other * capacity : (other + 1) * capacity
                ].astype(jnp.bfloat16)
        each_other(lambda other: deal(slab, other).start())
        arrived[slab, me] = sent[slab, me]

    def apply_expert(step, part):
        block = steps[step]
        for piece in range(SPLIT):
            slab = block * SPLIT + piece
            each_other(lambda other: landing(arrived, arrived_sem, slab, other).wait_recv())
            for other in range(members):
                wide_rows[
                    other * capacity : (other + 1) * capacity, piece * part_width : (piece + 1) * part_width
                ] = arrived[slab, other].astype(jnp.float32)
        rows = wide_rows[...].astype(jnp.bfloat16)
        gate = jnp.dot(rows, gate_w[0], preferred_element_type=jnp.float32)
        up = jnp.dot(rows, up_w[0], preferred_element_type=jnp.float32)
        hidden = (jax.nn.silu(gate) * up).astype(jnp.bfloat16)
        for piece in range(SHARE):
            slab = block * SHARE + piece
            for first in range(0, share_width, column):
                at = piece * share_width + first
                rows = jnp.dot(hidden, down_w[0, :, at : at + column], preferred_element_type=jnp.float32)
                for other in range(members):
                    replies[slab, other, :, first : first + column] = rows[
                        other * capacity : (other + 1) * capacity
                    ].astype(jnp.bfloat16)
            each_other(lambda other: reply(slab, other).start())
            returned[slab, me] = replies[slab, me]

    def combine(step, part):
        block = steps[step]
        slab = block * SHARE + part
        each_other(lambda other: landing(returned, returned_sem, slab, other).wait_recv())
        weights = mix_weights[block]
        for first in range(0, share_width, column):
            rows = jnp.concatenate(
                [returned[slab, other, :, first : first + column].astype(jnp.float32) for other in range(members)],
                axis=0,
            ).astype(jnp.bfloat16)
            both = lax.dot_general(
                weights, rows, (((0,), (0,)), ((), ())), preferred_element_type=jnp.float32
            )
            added = both[:row_count] + both[row_count:]
            if step == 0:
                at = part * share_width + first
                total[:, at : at + column] += added
            else:
                partial[slab, :, first : first + column] = added.astype(jnp.bfloat16)
                if joins and step > 1:
                    kept[(step - 2) * SHARE + part, :, first : first + column] = added
        if joins and step > 1:

            @pl.when(jnp.logical_not(inner))
            def _():
                join(block, step, part).start()

        elif step > 0:
            homeward(block, part).start()

    def merge(step, part):
        block = steps[step]
        slot = (step - 2) * SHARE + part

        @pl.when(inner)
        def _():
            join(block, step, part).wait_recv()
            partial[block * SHARE + part] = (kept[slot] + joined[slot].astype(jnp.float32)).astype(jnp.bfloat16)
            homeward(block, part).start()

    def shared(step, part):
        rows = hidden_ref[...]
        gate = jnp.dot(rows, sgate_w[...], preferred_element_type=jnp.float32)
        up = jnp.dot(rows, sup_w[...], preferred_element_type=jnp.float32)
        hidden = (jax.nn.silu(gate) * up).astype(jnp.bfloat16)
        for first in range(0, width, column):
            total[:, first : first + column] += jnp.dot(
                hidden, sdown_w[:, first : first + column], preferred_element_type=jnp.float32
            )

    place(plane)
    for load in loads[12:17]:
        load.wait()
    each_tp(lambda other: token_from(other).wait_recv())
    token_rows = jnp.concatenate([tokens[other] for other in range(tp_count)], axis=1)
    pre_gate = jnp.dot(token_rows, glu_w[...], preferred_element_type=jnp.float32) + bias_ref[...]
    gated = token_rows.astype(jnp.float32) * jax.nn.sigmoid(pre_gate)
    normed = rms_scale(gated, mix_gain_ref[...]).astype(jnp.bfloat16)
    stream = residual_ref[...].astype(jnp.float32) + jnp.dot(
        normed, proj_w[...], preferred_element_type=jnp.float32
    )
    total[...] = stream
    hidden = rms_scale(stream, norm_gain_ref[...]).astype(jnp.bfloat16)
    hidden_ref[...] = hidden
    for part in range(SPLIT):
        blocks[plane * SPLIT + part] = hidden[:, part * part_width : (part + 1) * part_width]
        forward(plane, part)
    for load in loads[17:]:
        load.wait()
    actions = {"A": dispatch, "F": relay, "S": shared, "B": apply_expert, "C": combine, "M": merge}
    for stage, step, part in stages_of(planes):
        actions[stage](step, part)
        if stage == "S":
            each_sp(lambda other: route_from(other).wait_recv())
            for later in steps[1:]:
                place(later)
    senders = [beside, jnp.where(plane < 2, 2, 1)] if joins else steps[1:]
    for part in range(SHARE):
        at = slice(part * share_width, (part + 1) * share_width)
        result = total[:, at]
        for source in senders:
            pltpu.make_async_remote_copy(
                src_ref=partial.at[source * SHARE + part],
                dst_ref=homed.at[source * SHARE + part],
                send_sem=partial_sem.at[source * SHARE + part],
                recv_sem=homed_sem.at[source * SHARE + part],
                device_id=plane_id(source),
                device_id_type=MESH,
            ).wait_recv()
            result = result + homed[source * SHARE + part].astype(jnp.float32)
        out_ref[:, at] = result.astype(out_ref.dtype)

    for step in range(planes):
        block = steps[step]
        for part in range(SPLIT):

            @pl.when(goes_up(block))
            def _():
                pass_up(block, part).wait_send()

            @pl.when(goes_down(block))
            def _():
                pass_down(block, part).wait_send()

            each_other(lambda other: deal(block * SPLIT + part, other).wait_send())
        for part in range(SHARE):
            each_other(lambda other: reply(block * SHARE + part, other).wait_send())
            if step > 0:
                homeward(block, part).wait_send()
    each_sp(lambda other: end_to(other).wait_send())
    each_sp(lambda other: route_to(other).wait_send())
    each_tp(lambda other: token_to(other).wait_send())


def layer(arguments, capacity, collective_id):
    sp_count, tp_count = lax.axis_size("sp"), lax.axis_size("tp")
    inputs, residual, input_re = arguments[0], arguments[1], arguments[5]
    length, channel_count = inputs.shape
    groups, channels, states = input_re.shape
    rows, width = residual.shape
    top_count = arguments[10].shape[0]
    wide = groups * states
    planes = planes_of(sp_count)
    members = sp_count * tp_count // planes
    capacity = -(-capacity // 8) * 8
    slots = members * capacity
    hbm = pl.BlockSpec(memory_space=pl.ANY)
    bf16, f32 = jnp.bfloat16, jnp.float32
    vmem, dma = pltpu.VMEM, pltpu.SemaphoreType.DMA
    pieces = vmem((planes * SPLIT, members, capacity, width // SPLIT), bf16)
    shares = vmem((planes * SHARE, members, capacity, width // SHARE), bf16)
    whole = vmem((planes * SPLIT, rows, width // SPLIT), bf16)
    parts = vmem((planes * SHARE, rows, width // SHARE), bf16)
    tables = vmem((2, channel_count, 2 * wide), bf16)
    tokens = vmem((tp_count, rows, channel_count), bf16)
    routes = (2 * top_count, rows)
    return pl.pallas_call(
        functools.partial(layer_kernel, sp_count, tp_count, capacity),
        out_shape=jax.ShapeDtypeStruct((rows, width), bf16),
        in_specs=[hbm] * len(arguments),
        out_specs=pl.BlockSpec(memory_space=pltpu.VMEM),
        scratch_shapes=[vmem(argument.shape, argument.dtype) for argument in arguments]
        + [
            tables,
            vmem((2 * wide, channel_count), bf16),
            vmem((length, 2 * wide), f32),
            vmem((length, channel_count), bf16),
            tokens,
            vmem((2, wide), f32),
            vmem((sp_count, 2, wide), f32),
            tokens,
            vmem(routes, f32),
            vmem((sp_count,) + routes, f32),
            vmem((planes, slots, rows), bf16),
            vmem((rows, width), bf16),
            whole,
            pieces,
            pieces,
            shares,
            shares,
            parts,
            parts,
            vmem((planes, slots, 2 * rows), bf16),
            vmem((2 * SHARE, rows, width // SHARE), f32),
            vmem((2 * SHARE, rows, width // SHARE), bf16),
            vmem((slots, width), f32),
            vmem((rows, width), f32),
            dma((len(arguments),)),
        ]
        + [dma((sp_count,))] * 4
        + [dma((tp_count,))] * 2
        + [dma((planes * SPLIT,))] * 3
        + [dma((planes * SPLIT, members))] * 2
        + [dma((planes * SHARE, members))] * 2
        + [dma((planes * SHARE,))] * 2
        + [dma((2 * SHARE,))],
        compiler_params=pltpu.CompilerParams(
            collective_id=collective_id, has_side_effects=True, vmem_limit_bytes=63 * 2**20
        ),
    )(*arguments)


def on_device(
    mixer_input,
    residual,
    decay_real,
    decay_imag,
    log_step,
    input_re,
    input_im,
    output_re,
    output_im,
    skip_gain,
    glu_weight,
    glu_bias,
    mix_gain,
    out_weight,
    norm_gain,
    route_ids,
    route_gates,
    expert_gate,
    expert_up,
    expert_down,
    shared_gate,
    shared_up,
    shared_down,
):
    row_count, top_count = route_ids.shape
    expert_count = lax.axis_size(("sp", "tp"))
    capacity = max(2, 3 * row_count * top_count // (2 * expert_count))
    arguments = (
        mixer_input,
        residual,
        decay_real,
        decay_imag,
        log_step[None, :],
        jnp.swapaxes(input_re, 1, 2),
        jnp.swapaxes(input_im, 1, 2),
        output_re,
        output_im,
        skip_gain,
        route_ids.T,
        route_gates.T,
        glu_weight,
        glu_bias[None, :],
        mix_gain[None, :],
        out_weight,
        norm_gain[None, :],
        shared_gate,
        shared_up,
        shared_down,
        expert_gate,
        expert_up,
        expert_down,
    )
    return layer(arguments, capacity, 1)


def solution(mesh):
    return jax.shard_map(
        on_device,
        mesh=mesh,
        in_specs=(
            P("sp", "tp"),
            P(("sp", "tp"), None),
            P("tp", None),
            P("tp", None),
            P("tp"),
            P("tp", None, None),
            P("tp", None, None),
            P("tp", None, None),
            P("tp", None, None),
            P("tp", None),
            P(),
            P(),
            P(),
            P(),
            P(),
            P(("sp", "tp"), None),
            P(("sp", "tp"), None),
            P(("sp", "tp"), None, None),
            P(("sp", "tp"), None, None),
            P(("sp", "tp"), None, None),
            P(),
            P(),
            P(),
        ),
        out_specs=P(("sp", "tp"), None),
        check_vma=False,
    )
```
